1024 devices in a mesh: grp: 2 (over x), sp: 16 (over z), tp: 32 (over y, core).
Axes of the slice: x: 2, y: 16, z: 16, core: 2. Of those that a mesh axis runs over, the one named last changes fastest.
The devices are a block of a 4x16x16 slice.
Arguments:
- tokens: bfloat16 [4, 4096, 2048], P('grp', 'sp'), parts along dimension 0, may hold values from -6 to 6
- decoded_input: bfloat16 [4, 2048], P('grp'), parts along dimension 0, may hold values from -6 to 6
- query_weight: bfloat16 [2048, 4096], P(None, 'tp'), may hold values from -0.125 to 0.125
- key_weight: bfloat16 [2048, 4096], P(None, 'tp'), may hold values from -0.125 to 0.125
- value_weight: bfloat16 [2048, 4096], P(None, 'tp'), may hold values from -0.125 to 0.125
- gate_weight: bfloat16 [2048, 2, 32], replicated, may hold values from -0.125 to 0.125
- head_decay_rate: float32 [32], P('tp'), may hold values from 2.4414063e-05 to 0.08, as said below
- extra_log_decay: float32 [4, 32, 4096], P('grp', 'tp', 'sp'), parts along dimension 0, may hold values from -2.8 to 0, as said below
- read_norm_gain: float32 [128], replicated, may hold values from 0.1 to 1.9
Outputs:
- cache: bfloat16 [4, 32, 128, 128], P('grp', 'tp', 'sp'), parts along dimension 0
- read: bfloat16 [4, 4096], P('grp', 'tp'), parts along dimension 0
The draws below stay inside these ranges and needn't reach their ends.
There are 2 independent parts, one for each index of `grp`. The reference program is written for one: setup_inputs(seed, part) draws one part's arguments, and reference() takes and returns one part's arrays. A program takes and returns all parts, laid end to end along the dimension named above; an argument that names none is the same for every part. Nothing has to cross between parts.
Inputs may be any that keep to these rules, and one draw needn't show every extreme that they name: `head_decay_rate`: positive. `extra_log_decay`: zero at all but a few positions.
All inputs are finite; a program needn't handle non-finite values.
Results may differ from the reference program's by a relative error of at most 0.002.
Values sent between devices are 32-bit elements; how exact they have to be, the bound alone decides.
A program may use at most 32 MiB of HBM per device.

```python
import jax
import jax.numpy as jnp
from jax import lax

D = 2048
H = 32
HEAD = 128
BLOCK = 64
SEQS = 2
LEN = 4096


def draw_head_decay_rate(key, part):
    span = 1.0 * LEN
    slow = jnp.exp(jax.random.uniform(jax.random.fold_in(key, 21), (H,), jnp.float32, jnp.log(0.1 / span), jnp.log(1.5 / span)))
    fast = jax.random.uniform(jax.random.fold_in(key, 22), (H,), jnp.float32, 0.02, 0.08)
    picked = jax.random.bernoulli(jax.random.fold_in(key, 23), 0.5, (H,))
    return jnp.where(picked, fast, slow).astype(jnp.float32)


def draw_extra_log_decay(key, part):
    places = jax.random.randint(jax.random.fold_in(key, 11), (SEQS, H, 4), 0, LEN)
    depths = jax.random.uniform(jax.random.fold_in(key, 12), (SEQS, H, 4), jnp.float32, jnp.log(0.5), jnp.log(0.8))
    where = jnp.arange(LEN)
    marks = jnp.where(where[None, None, None, :] == places[..., None], depths[..., None], 0.0)
    return jnp.sum(marks, axis=2).astype(jnp.float32)


def block_levels(own_key, shape, shards, low, high):
    level = 1.0
    for dim, parts in shards:
        heights = jax.random.uniform(jax.random.fold_in(jax.random.fold_in(own_key, 6), dim), (parts,), jnp.float32, low / len(shards), high / len(shards))
        level = level * jnp.repeat(jnp.exp(heights), shape[dim] // parts).reshape((-1,) + (1,) * (len(shape) - 1 - dim))
    return level


def scatter_about(stream_key, dims, scale, reach, pieces=(), kind=jnp.bfloat16):
    entries = jax.random.normal(stream_key, dims, jnp.float32) * scale
    if len(pieces) > 0:
        entries = block_levels(stream_key, dims, pieces, -0.22, 0.18) * entries
    return jnp.clip(entries, min=-reach, max=reach).astype(kind)


def setup_inputs(seed: int = 0, part: int = 0) -> dict:
    streams_of = jax.random.split(jax.random.key(seed), 10)
    own_keys = jax.random.split(jax.random.fold_in(streams_of[9], part), 10)
    tokens = scatter_about(own_keys[0], (SEQS, LEN, D), 1.0, 6.0, ((1, 16),))
    decoded_input = scatter_about(own_keys[1], (SEQS, D), 1.0, 6.0)
    query_weight = scatter_about(streams_of[2], (D, H * HEAD), D ** -0.5, 0.125, ((1, 32),))
    key_weight = scatter_about(streams_of[3], (D, H * HEAD), D ** -0.5, 0.125, ((1, 32),))
    value_weight = scatter_about(streams_of[4], (D, H * HEAD), D ** -0.5, 0.125, ((1, 32),))
    gate_weight = scatter_about(streams_of[5], (D, 2, H), D ** -0.5, 0.125)
    head_decay_rate = draw_head_decay_rate(jax.random.fold_in(streams_of[9], 71), part)
    extra_log_decay = draw_extra_log_decay(jax.random.fold_in(jax.random.fold_in(streams_of[9], part), 71), part)
    read_norm_gain = jnp.clip(1.0 + 0.18 * jax.random.normal(streams_of[8], (HEAD,), jnp.float32), 0.1, 1.9)
    return dict(tokens=tokens, decoded_input=decoded_input, query_weight=query_weight, key_weight=key_weight, value_weight=value_weight, gate_weight=gate_weight, head_decay_rate=head_decay_rate, extra_log_decay=extra_log_decay, read_norm_gain=read_norm_gain)


epsilon = 1e-06
write_offset = 5.0
highest = lax.Precision.HIGHEST

def unit_rows(vectors):
    return vectors * lax.rsqrt(lax.optimization_barrier(jnp.sum(vectors * vectors, axis=-1, keepdims=True)) + epsilon)

def project(flat, key_weight, value_weight, gate_cols, head_decay_rate, head_total, head_dim):
    keys = jax.nn.silu(jnp.dot(flat.astype(jnp.float32), key_weight.astype(jnp.float32), preferred_element_type=jnp.float32))
    keys = unit_rows(keys.reshape(flat.shape[0], head_total, head_dim))
    values = jax.nn.silu(jnp.dot(flat.astype(jnp.float32), value_weight.astype(jnp.float32), preferred_element_type=jnp.float32))
    values = values.reshape(flat.shape[0], head_total, head_dim)
    gates = jnp.dot(flat.astype(jnp.float32), gate_cols.astype(jnp.float32), preferred_element_type=jnp.float32)
    beta = jax.nn.sigmoid(gates[:, :head_total] - write_offset)
    decay_factor = -head_decay_rate * jax.nn.softplus(gates[:, head_total:])
    return (keys, values, beta, decay_factor)

def block_parts(keys, values, beta, decay_factor):
    size = keys.shape[-2]
    head_dim = values.shape[-1]
    running = jnp.cumsum(decay_factor, axis=-1)
    index = jnp.arange(size)
    strict = index[:, None] > index[None, :]
    spread = running[..., :, None] - running[..., None, :]
    below = jnp.where(strict, jnp.exp(jnp.where(strict, spread, 0.0)), 0.0)
    inner = jnp.einsum('...id,...jd->...ij', keys, keys, precision=highest)
    lower = jnp.eye(size, dtype=jnp.float32) + beta[..., :, None] * inner * below
    right = jnp.concatenate([values * beta[..., None], keys * (beta * jnp.exp(running))[..., None]], axis=-1)
    solved = jax.scipy.linalg.solve_triangular(lower, right, lower=True, unit_diagonal=True)
    total = jnp.exp(running[..., -1])
    carried = keys * jnp.exp(running[..., -1:] - running)[..., None]
    return (solved[..., :head_dim], solved[..., head_dim:], total, carried)

def reference(tokens, decoded_input, query_weight, key_weight, value_weight, gate_weight, head_decay_rate, extra_log_decay, read_norm_gain):
    sequence_total, prompt_length, width = tokens.shape
    head_total = head_decay_rate.shape[0]
    head_dim = key_weight.shape[1] // head_total
    gate_cols = gate_weight.reshape(width, 2 * head_total)
    flat = tokens.reshape(sequence_total * prompt_length, width)
    keys, values, beta, decay_factor = project(flat, key_weight, value_weight, gate_cols, head_decay_rate, head_total, head_dim)
    count = prompt_length // BLOCK
    keys_b = keys.reshape(sequence_total, count, BLOCK, head_total, head_dim).transpose(1, 0, 3, 2, 4)
    values_b = values.reshape(sequence_total, count, BLOCK, head_total, head_dim).transpose(1, 0, 3, 2, 4)
    beta_b = beta.reshape(sequence_total, count, BLOCK, head_total).transpose(1, 0, 3, 2)
    decay_every_token = decay_factor.reshape(sequence_total, prompt_length, head_total).transpose(0, 2, 1) + extra_log_decay
    decay_b = decay_every_token.reshape(sequence_total, head_total, count, BLOCK).transpose(2, 0, 1, 3)

    def advance(state, block):
        solved_u, solved_w, total, carried = block_parts(block[0], block[1], block[2], block[3])
        delta = solved_u - jnp.einsum('shcd,shdv->shcv', solved_w, state, precision=highest)
        state = total[..., None, None] * state + jnp.einsum('shcd,shcv->shdv', carried, delta, precision=highest)
        return (state, None)
    start = jnp.zeros((sequence_total, head_total, head_dim, head_dim), jnp.float32)
    final, _ = lax.scan(advance, start, (keys_b, values_b, beta_b, decay_b))
    query = jax.nn.silu(jnp.dot(decoded_input.astype(jnp.float32), query_weight.astype(jnp.float32), preferred_element_type=jnp.float32)).reshape(sequence_total, head_total, head_dim)
    new_key, new_value, new_beta, new_decay = project(decoded_input, key_weight, value_weight, gate_cols, head_decay_rate, head_total, head_dim)
    keep = jnp.exp(new_decay)
    key_read = jnp.einsum('shd,shdv->shv', new_key, final, precision=highest)
    query_read = jnp.einsum('shd,shdv->shv', query, final, precision=highest)
    intersection = lax.optimization_barrier(jnp.sum(query * new_key, axis=-1))
    cache = keep[..., None, None] * final - (keep * new_beta)[..., None, None] * new_key[..., :, None] * key_read[..., None, :] + new_beta[..., None, None] * new_key[..., :, None] * new_value[..., None, :]
    mixed = keep[..., None] * query_read - (keep * new_beta * intersection)[..., None] * key_read + (new_beta * intersection)[..., None] * new_value
    normed = mixed * lax.rsqrt(lax.optimization_barrier(jnp.mean(mixed * mixed, axis=-1, keepdims=True)) + epsilon) * read_norm_gain
    return (cache.astype(jnp.bfloat16), normed.reshape(sequence_total, head_total * head_dim).astype(jnp.bfloat16))
```

```python
import functools

import jax
import jax.numpy as jnp
from jax import lax
from jax.experimental import pallas as pl
from jax.experimental.pallas import tpu as pltpu
from jax.sharding import PartitionSpec as P

MESH = pl.DeviceIdType.MESH
F32 = jnp.float32
BF16 = jnp.bfloat16
epsilon = 1e-06
write_offset = 5.0
QUAD = 4


def split(x):
    hi = x.astype(BF16)
    lo = (x - hi.astype(F32)).astype(BF16)
    return hi, lo


def dot(a, b):
    return jnp.dot(a, b, preferred_element_type=F32)


def dot_nt(a, b):
    return lax.dot_general(a, b, (((1,), (1,)), ((), ())), preferred_element_type=F32)


def product(a, b, one=dot):
    ah, al = split(a)
    bh, bl = split(b)
    return one(ah, bh) + (one(ah, bl) + one(al, bh))


def silu(x):
    return x * jax.nn.sigmoid(x)


def softplus(x):
    return jnp.maximum(x, 0.0) + jnp.log1p(jnp.exp(-jnp.abs(x)))


def unit_rows(x):
    return x * lax.rsqrt(jnp.sum(x * x, axis=-1, keepdims=True) + epsilon)


def iota(shape, dim):
    return lax.broadcasted_iota(jnp.int32, shape, dim)


def kernel(
    seqs,
    rows,
    count,
    tok_hbm,
    dec_ref,
    wq_hbm,
    wk_hbm,
    wv_hbm,
    gate_ref,
    rate_ref,
    extra_ref,
    gain_ref,
    cache_ref,
    read_ref,
    x_ref,
    wkv_ref,
    wq_ref,
    k_ref,
    v_ref,
    n_ref,
    t_ref,
    ab_ref,
    rx1_ref,
    c1_ref,
    rx2_ref,
    c2_ref,
    rxa_ref,
    rxb_ref,
    ft_ref,
    tx_ref,
    tiles_ref,
    new_ref,
    load_sem,
    send1,
    recv1,
    send2,
    recv2,
    send_a,
    recv_a,
    send_b,
    recv_b,
    send_s,
    recv_s,
):
    me = lax.axis_index("sp")
    head = k_ref.shape[-1]
    mine = lax.rem(me, 2)
    quad = me // QUAD
    rank = lax.rem(me, QUAD)
    low = rank < 2
    is_even = mine == 0

    loads = [
        pltpu.make_async_copy(wk_hbm, wkv_ref.at[:, pl.ds(0, head)], load_sem.at[0]),
        pltpu.make_async_copy(wv_hbm, wkv_ref.at[:, pl.ds(head, head)], load_sem.at[1]),
    ]
    for s in range(seqs):
        loads.append(pltpu.make_async_copy(tok_hbm.at[s], x_ref.at[s], load_sem.at[2 + s]))
    loads.append(pltpu.make_async_copy(wq_hbm, wq_ref, load_sem.at[2 + seqs]))
    for load in loads:
        load.start()

    barrier = pltpu.get_barrier_semaphore()
    for k in range(1, count):
        pl.semaphore_signal(
            barrier, inc=1, device_id={"sp": lax.rem(me + k, count)}, device_id_type=MESH
        )

    loads[0].wait()
    loads[1].wait()

    gate_rows = []
    for s in range(seqs):
        loads[2 + s].wait()
        kv = silu(dot(x_ref[s], wkv_ref[...]))
        k_ref[s] = unit_rows(kv[:, :head])
        v_ref[s] = kv[:, head:]
        gate_rows.append(jnp.transpose(dot(x_ref[s], gate_ref[...])))
    rate = rate_ref[0]
    betas = [jax.nn.sigmoid(g[0:1] - write_offset) for g in gate_rows]
    decays = [-rate * softplus(g[1:2]) + extra_ref[s] for s, g in enumerate(gate_rows)]
    stacked = jnp.concatenate(decays, axis=0)
    hi, rest = split(stacked)
    rest32 = stacked - hi.astype(F32)
    lo = (rest32 - rest.astype(F32)).astype(BF16)
    row_i = iota((rows, rows), 0)
    col_i = iota((rows, rows), 1)
    upto = jnp.where(row_i <= col_i, 1.0, 0.0).astype(BF16)
    running = dot(hi, upto) + (dot(rest, upto) + dot(lo, upto))
    last = running[:, rows - 1 : rows]
    packed = jnp.concatenate(
        betas
        + [running, jnp.exp(running), jnp.exp(last - running)],
        axis=0,
    )
    columns = jnp.transpose(packed)

    def column(kind, s):
        at = kind * seqs + s
        return columns[:, at : at + 1]

    for s in range(seqs):
        keys = k_ref[s]
        inner = product(keys, keys, dot_nt)
        spread = column(1, s) - running[s : s + 1]
        strict = row_i > col_i
        below = jnp.where(strict, jnp.exp(jnp.where(strict, spread, 0.0)), 0.0)
        n_mat = column(0, s) * inner * below
        n_ref[s] = n_mat
        pair = jnp.logical_and(lax.shift_right_logical(row_i, 1) == lax.shift_right_logical(col_i, 1), strict)
        t_ref[s] = jnp.where(row_i == col_i, 1.0, 0.0) - jnp.where(pair, n_mat, 0.0)

    levels = rows.bit_length() - 1

    def level(at, carry):
        ri = lax.shift_right_logical(row_i, at)
        ci = lax.shift_right_logical(col_i, at)
        mask = jnp.logical_and(ri == ci + 1, lax.bitwise_and(ci, 1) == 0)
        for s in range(seqs):
            t_mat = t_ref[s]
            inner = product(jnp.where(mask, n_ref[s], 0.0), t_mat)
            t_ref[s] = t_mat - product(t_mat, inner)
        return carry

    lax.fori_loop(1, levels, level, 0)

    head_eye = jnp.where(iota((head, head), 0) == iota((head, head), 1), 1.0, 0.0)
    for s in range(seqs):
        keys = k_ref[s]
        right = jnp.concatenate(
            [keys * (column(0, s) * column(2, s)), v_ref[s] * column(0, s)], axis=1
        )
        solved = product(t_ref[s], right)
        both = product(jnp.transpose(solved), keys * column(3, s))
        ab_ref[s, :head] = jnp.exp(last[s : s + 1]) * head_eye - both[:head]
        ab_ref[s, head:] = both[head:]

    pl.semaphore_wait(barrier, count - 1)

    def other(flip):
        return {"sp": lax.bitwise_xor(me, flip)}

    copy1 = pltpu.make_async_remote_copy(
        src_ref=ab_ref.at[1 - mine],
        dst_ref=rx1_ref,
        send_sem=send1,
        recv_sem=recv1,
        device_id=other(1),
        device_id_type=MESH,
    )
    copy1.start()

    loads[2 + seqs].wait()
    dec = dec_ref[...]
    new_kv = silu(dot(dec, wkv_ref[...]))
    new_key = unit_rows(new_kv[:, :head])
    new_value = new_kv[:, head:]
    query = silu(dot(dec, wq_ref[...]))
    new_gate = dot(dec, gate_ref[...])
    new_beta = jax.nn.sigmoid(new_gate[:, 0:1] - write_offset)
    keep = jnp.exp(-rate * softplus(new_gate[:, 1:2]))
    for s in range(seqs):
        at = slice(s, s + 1)
        new_ref[s, 0:1] = new_key[at]
        new_ref[s, 1:2] = query[at]
        new_ref[s, 2:3] = new_value[at]
        new_ref[s, 3:4] = jnp.broadcast_to(new_beta[at], (1, head))
        new_ref[s, 4:5] = jnp.broadcast_to(keep[at], (1, head))
        new_ref[s, 5:8] = jnp.zeros((3, head), F32)

    copy1.wait()
    kept = ab_ref[mine]
    got = rx1_ref[...]
    left = jnp.where(is_even, kept, got)
    right = jnp.where(is_even, got, kept)
    both = product(left, right[:head])
    c1_ref[:head] = both[:head]
    c1_ref[head:] = both[head:] + right[head:]

    copy2 = pltpu.make_async_remote_copy(
        src_ref=c1_ref.at[pl.ds(pl.multiple_of(jnp.where(low, head, 0), head), head)],
        dst_ref=rx2_ref,
        send_sem=send2,
        recv_sem=recv2,
        device_id=other(2),
        device_id_type=MESH,
    )
    copy2.start()
    copy2.wait()
    own = c1_ref[:head]
    got = rx2_ref[...]
    both = product(jnp.where(low, own, got), jnp.where(low, got, own))
    c2_ref[...] = both + jnp.where(low, 0.0, c1_ref[head:])

    quads = count // QUAD
    share = head // quads

    def copy_a(k):
        return pltpu.make_async_remote_copy(
            src_ref=c2_ref,
            dst_ref=rxa_ref.at[quad],
            send_sem=send_a.at[k],
            recv_sem=recv_a.at[quad],
            device_id={"sp": lax.rem(quad + k, quads) * QUAD + rank},
            device_id_type=MESH,
        )

    def copy_b(k):
        to = lax.rem(quad + k, quads)
        return pltpu.make_async_remote_copy(
            src_ref=c2_ref.at[pl.ds(pl.multiple_of(to * share, share), share)],
            dst_ref=rxb_ref.at[quad],
            send_sem=send_b.at[k],
            recv_sem=recv_b.at[quad],
            device_id={"sp": to * QUAD + rank - 2},
            device_id_type=MESH,
        )

    far_first = sorted(range(quads), key=lambda k: -min(k, quads - k))

    @pl.when(jnp.logical_and(low, quad > 0))
    def _():
        for k in far_first:
            if k:
                copy_a(k).start()

    @pl.when(jnp.logical_not(low))
    def _():
        for k in far_first:
            copy_b(k).start()

    def arrival(ref, slot, sem, shape_ref):
        return pltpu.make_async_remote_copy(
            src_ref=shape_ref,
            dst_ref=ref.at[slot],
            send_sem=send1,
            recv_sem=sem.at[slot],
            device_id=other(1),
            device_id_type=MESH,
        )

    slot_mine = mine * quads + quad

    def copy_s(k):
        to = lax.rem(me + k, count)
        return pltpu.make_async_remote_copy(
            src_ref=tx_ref.at[pl.ds(pl.multiple_of(to * 8, 8), 8)],
            dst_ref=tiles_ref.at[slot_mine],
            send_sem=send_s.at[k],
            recv_sem=recv_s.at[slot_mine],
            device_id={"sp": to},
            device_id_type=MESH,
        )

    lane = iota((1, head), 1)

    @pl.when(low)
    def _():
        rxa_ref[quad] = c2_ref[...]
        arrival(rxb_ref, 0, recv_b, c2_ref.at[pl.ds(0, share)]).wait_recv()
        state = rxb_ref[0]
        for g in range(1, quads):

            @pl.when(quad != g)
            def _():
                arrival(rxa_ref, g, recv_a, c2_ref).wait_recv()

            arrival(rxb_ref, g, recv_b, c2_ref.at[pl.ds(0, share)]).wait_recv()
            state = product(state, rxa_ref[g]) + rxb_ref[g]
        ft_ref[...] = jnp.zeros((head, head), F32)
        ft_ref[pl.ds(pl.multiple_of(quad * share, share), share)] = state
        final = jnp.transpose(ft_ref[...])
        new = new_ref[mine]
        reads = product(new, final)
        key_read, query_read = reads[0:1], reads[1:2]
        beta, hold = new[3:4], new[4:5]
        value = jnp.where(lane // share == quad, new[2:3], 0.0)
        inter = jnp.sum(new[0:1] * new[1:2], axis=-1, keepdims=True)
        key_col = jnp.transpose(new)[:, 0:1]
        cache = hold * final - (hold * beta) * key_col * key_read + beta * key_col * value
        mixed = hold * query_read - (hold * beta * inter) * key_read + (beta * inter) * value
        moved = pltpu.roll(jnp.broadcast_to(mixed, (8, head)), share, 1)[0:1]
        first = lax.bitwise_and(iota((head, head), 0), 7) == 0
        tx_ref[...] = cache + jnp.where(first, moved, 0.0)
        tiles_ref[slot_mine] = tx_ref[pl.ds(pl.multiple_of(me * 8, 8), 8)]
        for k in sorted(range(1, count), key=lambda k: -min(k, count - k)):
            copy_s(k).start()

    for s in range(seqs):
        cache = jnp.zeros((8, head), F32)
        mixed = jnp.zeros((8, head), F32)
        for g in range(quads):

            @pl.when(me != g * QUAD + s)
            def _():
                arrival(tiles_ref, s * quads + g, recv_s, tx_ref.at[pl.ds(0, 8)]).wait_recv()

            tile = tiles_ref[s * quads + g]
            cache = cache + jnp.where(lane // share == g, tile, 0.0)
            mixed = mixed + jnp.where(lane // share == (g + 1) % quads, tile, 0.0)
        cache_ref[s, 0] = cache.astype(BF16)
        row = pltpu.roll(mixed, head - share, 1)[0:1]
        scale = lax.rsqrt(jnp.sum(row * row, axis=-1, keepdims=True) / head + epsilon)
        read_ref[s : s + 1] = (row * scale * gain_ref[...]).astype(BF16)

    @pl.when(jnp.logical_and(low, quad > 0))
    def _():
        for k in range(1, quads):
            copy_a(k).wait_send()

    @pl.when(jnp.logical_not(low))
    def _():
        for k in range(quads):
            copy_b(k).wait_send()

    @pl.when(low)
    def _():
        for k in range(1, count):
            copy_s(k).wait_send()


def per_device(
    tokens,
    decoded_input,
    query_weight,
    key_weight,
    value_weight,
    gate_weight,
    head_decay_rate,
    extra_log_decay,
    read_norm_gain,
):
    seqs, rows, width = tokens.shape
    head = key_weight.shape[1]
    count = lax.axis_size("sp")
    quads = count // QUAD
    gates = lax.dynamic_slice_in_dim(gate_weight, lax.axis_index("tp"), 1, 2)[:, :, 0]
    vmem = pl.BlockSpec(memory_space=pltpu.VMEM)
    hbm = pl.BlockSpec(memory_space=pl.ANY)
    dma = pltpu.SemaphoreType.DMA
    return pl.pallas_call(
        functools.partial(kernel, seqs, rows, count),
        out_shape=(
            jax.ShapeDtypeStruct((seqs, 1, head // count, head), BF16),
            jax.ShapeDtypeStruct((seqs, head), BF16),
        ),
        in_specs=[
            hbm,
            vmem,
            hbm,
            hbm,
            hbm,
            vmem,
            pl.BlockSpec(memory_space=pltpu.SMEM),
            vmem,
            vmem,
        ],
        out_specs=(vmem, vmem),
        scratch_shapes=[
            pltpu.VMEM((seqs, rows, width), BF16),
            pltpu.VMEM((width, 2 * head), BF16),
            pltpu.VMEM((width, head), BF16),
            pltpu.VMEM((seqs, rows, head), F32),
            pltpu.VMEM((seqs, rows, head), F32),
            pltpu.VMEM((seqs, rows, rows), F32),
            pltpu.VMEM((seqs, rows, rows), F32),
            pltpu.VMEM((seqs, 2 * head, head), F32),
            pltpu.VMEM((2 * head, head), F32),
            pltpu.VMEM((2 * head, head), F32),
            pltpu.VMEM((head, head), F32),
            pltpu.VMEM((head, head), F32),
            pltpu.VMEM((quads, head, head), F32),
            pltpu.VMEM((quads, head // quads, head), F32),
            pltpu.VMEM((head, head), F32),
            pltpu.VMEM((head, head), F32),
            pltpu.VMEM((seqs * quads, head // count, head), F32),
            pltpu.VMEM((seqs, 8, head), F32),
            dma((3 + seqs,)),
            dma,
            dma,
            dma,
            dma,
            dma((quads,)),
            dma((quads,)),
            dma((quads,)),
            dma((quads,)),
            dma((count,)),
            dma((seqs * quads,)),
        ],
        compiler_params=pltpu.CompilerParams(collective_id=0, has_side_effects=True),
    )(
        tokens,
        decoded_input,
        query_weight,
        key_weight,
        value_weight,
        gates,
        head_decay_rate,
        extra_log_decay,
        read_norm_gain.reshape(1, head),
    )


def solution(mesh):
    in_specs = (
        P("grp", "sp", None),
        P("grp", None),
        P(None, "tp"),
        P(None, "tp"),
        P(None, "tp"),
        P(),
        P("tp"),
        P("grp", "tp", "sp"),
        P(),
    )
    out_specs = (P("grp", "tp", "sp", None), P("grp", "tp"))
    return jax.shard_map(
        per_device, mesh=mesh, in_specs=in_specs, out_specs=out_specs, check_vma=False
    )
```

```python
import functools

import jax
import jax.numpy as jnp
from jax import lax
from jax.experimental import pallas as pl
from jax.experimental.pallas import tpu as pltpu
from jax.sharding import PartitionSpec as P

MESH = pl.DeviceIdType.MESH
F32 = jnp.float32
BF16 = jnp.bfloat16
epsilon = 1e-06
write_offset = 5.0


def split(x):
    hi = x.astype(BF16)
    lo = (x - hi.astype(F32)).astype(BF16)
    return hi, lo


def dot(a, b):
    return jnp.dot(a, b, preferred_element_type=F32)


def dot_nt(a, b):
    return lax.dot_general(a, b, (((1,), (1,)), ((), ())), preferred_element_type=F32)


def product(a, b, one=dot):
    ah, al = split(a)
    bh, bl = split(b)
    return one(ah, bh) + (one(ah, bl) + one(al, bh))


def silu(x):
    return x * jax.nn.sigmoid(x)


def softplus(x):
    return jnp.maximum(x, 0.0) + jnp.log1p(jnp.exp(-jnp.abs(x)))


def unit_rows(x):
    return x * lax.rsqrt(jnp.sum(x * x, axis=-1, keepdims=True) + epsilon)


def iota(shape, dim):
    return lax.broadcasted_iota(jnp.int32, shape, dim)


def kernel(
    seqs,
    rows,
    count,
    tok_hbm,
    dec_hbm,
    wq_hbm,
    wk_hbm,
    wv_hbm,
    gate_hbm,
    rate_hbm,
    extra_hbm,
    gain_hbm,
    cache_ref,
    read_ref,
    x_ref,
    dec_ref,
    wkv_ref,
    wq_ref,
    gate_ref,
    rate_ref,
    extra_ref,
    gain_ref,
    k_ref,
    v_ref,
    n_ref,
    t_ref,
    ab_ref,
    rx_ref,
    tx_ref,
    first_ref,
    new_tx,
    new_rx,
    out_tx,
    out_rx,
    load_sem,
    send_x,
    recv_x,
    send_f,
    recv_f,
    send_n,
    recv_n,
    send_o,
    recv_o,
):
    me = lax.axis_index("sp")
    head_index = lax.axis_index("tp")
    head = k_ref.shape[-1]
    gates = gate_ref.shape[0] // 2
    last_one = count - 1
    is_first = me == 0
    is_second = me == 1
    is_last = me == last_one
    in_chain = jnp.logical_and(me > 0, me < last_one)

    def load(source, target, place):
        copy = pltpu.make_async_copy(source, target, load_sem.at[place])
        copy.start()
        return copy

    load_w = [
        load(wk_hbm, wkv_ref.at[:, pl.ds(0, head)], 0),
        load(wv_hbm, wkv_ref.at[:, pl.ds(head, head)], 1),
    ]
    load_x = [load(tok_hbm.at[0], x_ref.at[0], 2)]
    load_g = [
        load(gate_hbm, gate_ref, 3),
        load(rate_hbm, rate_ref, 4),
        load(extra_hbm, extra_ref, 5),
    ]
    for s in range(1, seqs):
        load_x.append(load(tok_hbm.at[s], x_ref.at[s], 8 + s))
    load_r = load(gain_hbm, gain_ref, 6)

    def at(index):
        return {"sp": index}

    barrier = pltpu.get_barrier_semaphore()

    def greet(index):
        pl.semaphore_signal(barrier, inc=1, device_id=at(index), device_id_type=MESH)

    @pl.when(me >= 2)
    def _():
        greet(me - 1)

    @pl.when(is_last)
    def _():
        greet(0)
        greet(1)

    @pl.when(jnp.logical_not(is_last))
    def _():
        greet(last_one)

    for copy in load_w:
        copy.wait()

    row_g = iota((gates, rows), 0)
    gate_rows = []
    for s in range(seqs):
        load_x[s].wait()
        kv = silu(dot(x_ref[s], wkv_ref[...]))
        k_ref[s] = unit_rows(kv[:, :head])
        v_ref[s] = kv[:, head:]
        if s == 0:
            for copy in load_g:
                copy.wait()
        both = dot_nt(gate_ref[...], x_ref[s])
        picked = [
            jnp.sum(jnp.where(row_g == head_index, part, 0.0), axis=0, keepdims=True)
            for part in (both[:gates], both[gates:])
        ]
        gate_rows.append(picked)
    rate = rate_ref[...]
    betas = [jax.nn.sigmoid(g[0] - write_offset) for g in gate_rows]
    decays = [-rate * softplus(g[1]) + extra_ref[s] for s, g in enumerate(gate_rows)]
    stacked = jnp.concatenate(decays, axis=0)
    hi, rest = split(stacked)
    rest32 = stacked - hi.astype(F32)
    lo = (rest32 - rest.astype(F32)).astype(BF16)
    row_i = iota((rows, rows), 0)
    col_i = iota((rows, rows), 1)
    upto = jnp.where(row_i <= col_i, 1.0, 0.0).astype(BF16)
    running = dot(hi, upto) + (dot(rest, upto) + dot(lo, upto))
    last = running[:, rows - 1 : rows]
    packed = jnp.concatenate(
        betas + [running, jnp.exp(running), jnp.exp(last - running)],
        axis=0,
    )
    columns = jnp.transpose(packed)

    def column(kind, s):
        place = kind * seqs + s
        return columns[:, place : place + 1]

    strict = row_i > col_i
    pair = jnp.logical_and(
        lax.shift_right_logical(row_i, 1) == lax.shift_right_logical(col_i, 1), strict
    )
    for s in range(seqs):
        keys = k_ref[s]
        inner = product(keys, keys, dot_nt)
        spread = column(1, s) - running[s : s + 1]
        below = jnp.where(strict, jnp.exp(jnp.where(strict, spread, 0.0)), 0.0)
        n_mat = column(0, s) * inner * below
        n_ref[s] = n_mat
        t_ref[s] = jnp.where(row_i == col_i, 1.0, 0.0) - jnp.where(pair, n_mat, 0.0)

    levels = rows.bit_length() - 1

    def level(depth, carry):
        ri = lax.shift_right_logical(row_i, depth)
        ci = lax.shift_right_logical(col_i, depth)
        mask = jnp.logical_and(ri == ci + 1, lax.bitwise_and(ci, 1) == 0)
        for s in range(seqs):
            t_mat = t_ref[s]
            inner = product(jnp.where(mask, n_ref[s], 0.0), t_mat)
            t_ref[s] = t_mat - product(t_mat, inner)
        return carry

    lax.fori_loop(1, levels, level, 0)

    head_eye = jnp.where(iota((head, head), 0) == iota((head, head), 1), 1.0, 0.0)
    for s in range(seqs):
        keys = k_ref[s]
        right = jnp.concatenate(
            [keys * (column(0, s) * column(2, s)), v_ref[s] * column(0, s)], axis=1
        )
        solved = product(t_ref[s], right)
        both = product(jnp.transpose(solved), keys * column(3, s))
        ab_ref[s, 0] = jnp.exp(last[s : s + 1]) * head_eye - both[:head]
        ab_ref[s, 1] = both[head:]

    chunks = [(s, half) for s in range(seqs) for half in range(2)]

    def chain(s, half, source):
        return pltpu.make_async_remote_copy(
            src_ref=source.at[s, half],
            dst_ref=rx_ref.at[s, half],
            send_sem=send_x.at[s, half],
            recv_sem=recv_x.at[s, half],
            device_id=at(lax.rem(me + 1, count)),
            device_id_type=MESH,
        )

    def push(s):
        return pltpu.make_async_remote_copy(
            src_ref=ab_ref.at[s, 1],
            dst_ref=first_ref.at[s],
            send_sem=send_f.at[s],
            recv_sem=recv_f.at[s],
            device_id=at(last_one),
            device_id_type=MESH,
        )

    decoded = pltpu.make_async_remote_copy(
        src_ref=new_tx,
        dst_ref=new_rx,
        send_sem=send_n,
        recv_sem=recv_n,
        device_id=at(last_one),
        device_id_type=MESH,
    )

    def rows_to(s, k):
        to = lax.rem(me + k, count)
        return pltpu.make_async_remote_copy(
            src_ref=out_tx.at[s, to],
            dst_ref=out_rx.at[s],
            send_sem=send_o.at[s, k],
            recv_sem=recv_o.at[s],
            device_id=at(to),
            device_id_type=MESH,
        )

    @pl.when(is_first)
    def _():
        pl.semaphore_wait(barrier, 1)
        for s in range(seqs):
            push(s).start()

    @pl.when(is_second)
    def _():
        pl.semaphore_wait(barrier, 2)
        for s, half in chunks:
            chain(s, half, ab_ref).start()
        copies = [
            pltpu.make_async_copy(dec_hbm, dec_ref, load_sem.at[7]),
            pltpu.make_async_copy(wq_hbm, wq_ref, load_sem.at[8]),
        ]
        for copy in copies:
            copy.start()
        for copy in copies:
            copy.wait()
        dec = dec_ref[...]
        new_kv = silu(dot(dec, wkv_ref[...]))
        new_key = unit_rows(new_kv[:, :head])
        new_value = new_kv[:, head:]
        query = silu(dot(dec, wq_ref[...]))
        both = dot_nt(gate_ref[...], dec)
        row_n = iota((gates, seqs), 0)
        picked = [
            jnp.sum(jnp.where(row_n == head_index, part, 0.0), axis=0, keepdims=True)
            for part in (both[:gates], both[gates:])
        ]
        new_beta = jax.nn.sigmoid(picked[0] - write_offset)
        keep = jnp.exp(-rate * softplus(picked[1]))
        for s in range(seqs):
            one = slice(s, s + 1)
            new_tx[s, 0:1] = new_key[one]
            new_tx[s, 1:2] = query[one]
            new_tx[s, 2:3] = new_value[one]
            new_tx[s, 3:4] = jnp.broadcast_to(new_beta[:, one], (1, head))
            new_tx[s, 4:5] = jnp.broadcast_to(keep[:, one], (1, head))
            new_tx[s, 5:8] = jnp.zeros((3, head), F32)
        decoded.start()

    @pl.when(jnp.logical_and(in_chain, me >= 2))
    def _():
        pl.semaphore_wait(barrier, 1)
        for s, half in chunks:
            chain(s, half, tx_ref).wait_recv()
            moved = product(rx_ref[s, half], ab_ref[s, 0])
            if half == 1:
                moved = moved + ab_ref[s, 1]
            tx_ref[s, half] = moved
            chain(s, half, tx_ref).start()

    @pl.when(is_last)
    def _():
        pl.semaphore_wait(barrier, count - 1)
        load_r.wait()
        decoded.wait_recv()
        for s in range(seqs):
            push(s).wait_recv()
            chain(s, 0, tx_ref).wait_recv()
            joined = product(first_ref[s], rx_ref[s, 0])
            chain(s, 1, tx_ref).wait_recv()
            joined = joined + rx_ref[s, 1]
            flipped = product(joined, ab_ref[s, 0]) + ab_ref[s, 1]
            new = new_rx[s]
            reads = product(new, flipped, dot_nt)
            final = jnp.transpose(flipped)
            key_read, query_read = reads[0:1], reads[1:2]
            value, beta, hold = new[2:3], new[3:4], new[4:5]
            inter = jnp.sum(new[0:1] * new[1:2], axis=-1, keepdims=True)
            key_col = jnp.transpose(new)[:, 0:1]
            cache = hold * final + key_col * (beta * value - (hold * beta) * key_read)
            mixed = hold * query_read - (hold * beta * inter) * key_read + (beta * inter) * value
            scale = lax.rsqrt(jnp.sum(mixed * mixed, axis=-1, keepdims=True) / head + epsilon)
            read = mixed * scale * gain_ref[...]
            each = head // count
            out_tx[s, :, :each] = cache.reshape(count, each, head)
            out_tx[s, :, each:] = jnp.broadcast_to(read.reshape(1, 1, head), (count, each, head))
            for k in range(1, count):
                rows_to(s, k).start()
            out_rx[s] = out_tx[s, last_one]

    for s in range(seqs):

        @pl.when(jnp.logical_not(is_last))
        def _():
            rows_to(s, 1).wait_recv()

        each = head // count
        cache_ref[s, 0] = out_rx[s, :each].astype(BF16)
        read_ref[s : s + 1] = out_rx[s, each : each + 1].astype(BF16)

    @pl.when(jnp.logical_not(is_last))
    def _():
        load_r.wait()

    @pl.when(is_first)
    def _():
        for s in range(seqs):
            push(s).wait_send()

    @pl.when(in_chain)
    def _():
        for s, half in chunks:
            chain(s, half, tx_ref).wait_send()

    @pl.when(is_second)
    def _():
        decoded.wait_send()

    @pl.when(is_last)
    def _():
        for s in range(seqs):
            for k in range(1, count):
                rows_to(s, k).wait_send()


def per_device(
    tokens,
    decoded_input,
    query_weight,
    key_weight,
    value_weight,
    gate_weight,
    head_decay_rate,
    extra_log_decay,
    read_norm_gain,
):
    seqs, rows, width = tokens.shape
    head = key_weight.shape[1]
    count = lax.axis_size("sp")
    each = head // count
    gates = gate_weight.transpose(1, 2, 0).reshape(-1, width)
    vmem = pl.BlockSpec(memory_space=pltpu.VMEM)
    hbm = pl.BlockSpec(memory_space=pl.ANY)
    dma = pltpu.SemaphoreType.DMA
    return pl.pallas_call(
        functools.partial(kernel, seqs, rows, count),
        out_shape=(
            jax.ShapeDtypeStruct((seqs, 1, each, head), BF16),
            jax.ShapeDtypeStruct((seqs, head), BF16),
        ),
        in_specs=[hbm] * 9,
        out_specs=(vmem, vmem),
        scratch_shapes=[
            pltpu.VMEM((seqs, rows, width), BF16),
            pltpu.VMEM((seqs, width), BF16),
            pltpu.VMEM((width, 2 * head), BF16),
            pltpu.VMEM((width, head), BF16),
            pltpu.VMEM(gates.shape, BF16),
            pltpu.VMEM((1, 1), F32),
            pltpu.VMEM((seqs, 1, rows), F32),
            pltpu.VMEM((1, head), F32),
            pltpu.VMEM((seqs, rows, head), F32),
            pltpu.VMEM((seqs, rows, head), F32),
            pltpu.VMEM((seqs, rows, rows), F32),
            pltpu.VMEM((seqs, rows, rows), F32),
            pltpu.VMEM((seqs, 2, head, head), F32),
            pltpu.VMEM((seqs, 2, head, head), F32),
            pltpu.VMEM((seqs, 2, head, head), F32),
            pltpu.VMEM((seqs, head, head), F32),
            pltpu.VMEM((seqs, 8, head), F32),
            pltpu.VMEM((seqs, 8, head), F32),
            pltpu.VMEM((seqs, count, 2 * each, head), F32),
            pltpu.VMEM((seqs, 2 * each, head), F32),
            dma((8 + seqs,)),
            dma((seqs, 2)),
            dma((seqs, 2)),
            dma((seqs,)),
            dma((seqs,)),
            dma,
            dma,
            dma((seqs, count)),
            dma((seqs,)),
        ],
        compiler_params=pltpu.CompilerParams(collective_id=0, has_side_effects=True),
    )(
        tokens,
        decoded_input,
        query_weight,
        key_weight,
        value_weight,
        gates,
        head_decay_rate.reshape(1, 1),
        extra_log_decay,
        read_norm_gain.reshape(1, head),
    )


def solution(mesh):
    in_specs = (
        P("grp", "sp", None),
        P("grp", None),
        P(None, "tp"),
        P(None, "tp"),
        P(None, "tp"),
        P(),
        P("tp"),
        P("grp", "tp", "sp"),
        P(),
    )
    out_specs = (P("grp", "tp", "sp", None), P("grp", "tp"))
    return jax.shard_map(
        per_device, mesh=mesh, in_specs=in_specs, out_specs=out_specs, check_vma=False
    )
```

```python
import functools

import jax
import jax.numpy as jnp
from jax import lax
from jax.experimental import pallas as pl
from jax.experimental.pallas import tpu as pltpu
from jax.sharding import PartitionSpec as P

MESH = pl.DeviceIdType.MESH
F32 = jnp.float32
BF16 = jnp.bfloat16
epsilon = 1e-06
write_offset = 5.0
BLOCK = 64


def split(x):
    hi = x.astype(BF16)
    lo = (x - hi.astype(F32)).astype(BF16)
    return hi, lo


def dot(a, b):
    return jnp.dot(a, b, preferred_element_type=F32)


def dot_nt(a, b):
    return lax.dot_general(a, b, (((1,), (1,)), ((), ())), preferred_element_type=F32)


def passes(a, b, one=dot):
    return one(a[0], b[0]) + (one(a[0], b[1]) + one(a[1], b[0]))


def product(a, b, one=dot):
    return passes(split(a), split(b), one)


def silu(x):
    return x * jax.nn.sigmoid(x)


def softplus(x):
    return jnp.maximum(x, 0.0) + jnp.log1p(jnp.exp(-jnp.abs(x)))


def unit_rows(x):
    return x * lax.rsqrt(jnp.sum(x * x, axis=-1, keepdims=True) + epsilon)


def iota(shape, dim):
    return lax.broadcasted_iota(jnp.int32, shape, dim)


def kernel(
    seqs,
    rows,
    count,
    tok_hbm,
    dec_hbm,
    wq_hbm,
    wk_hbm,
    wv_hbm,
    gate_hbm,
    rate_hbm,
    extra_hbm,
    gain_hbm,
    cache_ref,
    read_ref,
    x_ref,
    dec_ref,
    wkv_ref,
    wq_ref,
    gate_ref,
    rate_ref,
    extra_ref,
    gain_ref,
    k_ref,
    v_ref,
    ab_ref,
    rx_ref,
    tx_ref,
    first_ref,
    new_tx,
    new_rx,
    out_tx,
    out_rx,
    load_sem,
    send_x,
    recv_x,
    send_f,
    recv_f,
    send_n,
    recv_n,
    send_o,
    recv_o,
):
    me = lax.axis_index("sp")
    head_index = lax.axis_index("tp")
    head = k_ref.shape[-1]
    gates = gate_ref.shape[0] // 2
    last_one = count - 1
    is_first = me == 0
    is_second = me == 1
    is_last = me == last_one
    in_chain = jnp.logical_and(me > 0, me < last_one)

    def load(source, target, place):
        copy = pltpu.make_async_copy(source, target, load_sem.at[place])
        copy.start()
        return copy

    load_w = [
        load(wk_hbm, wkv_ref.at[:, pl.ds(0, head)], 0),
        load(wv_hbm, wkv_ref.at[:, pl.ds(head, head)], 1),
    ]
    load_x = [load(tok_hbm.at[0], x_ref.at[0], 2)]
    load_g = [
        load(gate_hbm, gate_ref, 3),
        load(rate_hbm, rate_ref, 4),
        load(extra_hbm, extra_ref, 5),
    ]
    for s in range(1, seqs):
        load_x.append(load(tok_hbm.at[s], x_ref.at[s], 8 + s))
    load_r = load(gain_hbm, gain_ref, 6)

    def at(index):
        return {"sp": index}

    barrier = pltpu.get_barrier_semaphore()

    def greet(index):
        pl.semaphore_signal(barrier, inc=1, device_id=at(index), device_id_type=MESH)

    @pl.when(me >= 2)
    def _():
        greet(me - 1)

    @pl.when(is_last)
    def _():
        greet(0)
        greet(1)

    @pl.when(jnp.logical_not(is_last))
    def _():
        greet(last_one)

    for copy in load_w:
        copy.wait()

    row_g = iota((gates, rows), 0)
    gate_rows = []
    for s in range(seqs):
        load_x[s].wait()
        kv = silu(dot(x_ref[s], wkv_ref[...]))
        k_ref[s] = unit_rows(kv[:, :head])
        v_ref[s] = kv[:, head:]
        if s == 0:
            for copy in load_g:
                copy.wait()
        both = dot_nt(gate_ref[...], x_ref[s])
        picked = [
            jnp.sum(jnp.where(row_g == head_index, part, 0.0), axis=0, keepdims=True)
            for part in (both[:gates], both[gates:])
        ]
        gate_rows.append(picked)
    rate = rate_ref[...]
    betas = [jax.nn.sigmoid(g[0] - write_offset) for g in gate_rows]
    decays = [-rate * softplus(g[1]) + extra_ref[s] for s, g in enumerate(gate_rows)]
    stacked = jnp.concatenate(decays, axis=0)
    hi, rest = split(stacked)
    rest32 = stacked - hi.astype(F32)
    lo = (rest32 - rest.astype(F32)).astype(BF16)
    parts = (hi, rest, lo)
    row_i = iota((rows, rows), 0)
    col_i = iota((rows, rows), 1)
    together = row_i // BLOCK == col_i // BLOCK
    upto = jnp.where(jnp.logical_and(together, row_i <= col_i), 1.0, 0.0).astype(BF16)
    whole = jnp.where(together, 1.0, 0.0).astype(BF16)
    running = sum(dot(part, upto) for part in parts)
    total = sum(dot(part, whole) for part in parts)
    grown = jnp.exp(running)
    packed = jnp.concatenate(
        betas
        + [running]
        + [betas[s] * grown[s : s + 1] for s in range(seqs)]
        + [jnp.exp(total - running)],
        axis=0,
    )
    columns = jnp.transpose(packed)

    def column(kind, s):
        place = kind * seqs + s
        return columns[:, place : place + 1]

    blocks = rows // BLOCK
    row_c = iota((BLOCK, rows), 0)
    lane_c = iota((BLOCK, rows), 1)
    inside = lax.bitwise_and(lane_c, BLOCK - 1)
    owner = lane_c // BLOCK
    own_lanes = [jnp.where(owner == b, 1.0, 0.0).astype(BF16) for b in range(blocks)]
    strict = row_c > inside
    eye = jnp.where(row_c == inside, 1.0, 0.0)

    def compact(full):
        out = jnp.where(owner == 0, full[:BLOCK], 0.0)
        for b in range(1, blocks):
            out = jnp.where(owner == b, full[b * BLOCK : (b + 1) * BLOCK], out)
        return out

    def diagonal(pair):
        return [jnp.concatenate([part * own for own in own_lanes], axis=0) for part in pair]

    n_mats, solves = [], []
    for s in range(seqs):
        halves = split(k_ref[s])
        inner = compact(passes(halves, halves, dot_nt))
        spread = compact(jnp.broadcast_to(column(1, s), (rows, rows))) - running[s : s + 1]
        below = jnp.where(strict, jnp.exp(jnp.where(strict, spread, 0.0)), 0.0)
        n_mat = compact(jnp.broadcast_to(column(0, s), (rows, rows))) * inner * below
        pair = row_c // 2 == inside // 2
        n_mats.append(n_mat)
        solves.append(eye - jnp.where(pair, n_mat, 0.0))
    depth = 1
    while 1 << depth < BLOCK:
        ri = lax.shift_right_logical(row_c, depth)
        ci = lax.shift_right_logical(inside, depth)
        mask = jnp.logical_and(ri == ci + 1, lax.bitwise_and(ci, 1) == 0)
        for s in range(seqs):
            t_mat = split(solves[s])
            inner = passes(split(jnp.where(mask, n_mats[s], 0.0)), diagonal(t_mat))
            solves[s] = solves[s] - passes(t_mat, diagonal(split(inner)))
        depth += 1

    head_eye = jnp.where(iota((head, head), 0) == iota((head, head), 1), 1.0, 0.0)
    row_b = iota((rows, 1), 0) // BLOCK
    inverse = [diagonal(split(t_mat)) for t_mat in solves]
    carried, steps = [], []
    for s in range(seqs):
        keys = k_ref[s]
        weights = passes(inverse[s], split(keys * column(2, s)))
        kept = keys * column(3, s)
        spans = jnp.concatenate(
            [jnp.where(row_b == b, kept, 0.0) for b in range(blocks)], axis=1
        )
        carried.append(split(spans))
        moved = passes(split(jnp.transpose(weights)), carried[s])
        step = []
        for b in range(blocks):
            decay = jnp.exp(total[s : s + 1, b * BLOCK : b * BLOCK + 1])
            step.append(split(decay * head_eye - moved[:, b * head : (b + 1) * head]))
        steps.append(step)
    tails = []
    for s in range(seqs):
        step = steps[s]
        tail = split(passes(step[2], step[3]))
        tails.append(tail)
        ab_ref[s, 0] = passes(split(passes(step[0], step[1])), tail)

    def pushes():
        for s in range(seqs):
            deltas = passes(inverse[s], split(v_ref[s] * column(0, s)))
            moved = passes(split(jnp.transpose(deltas)), carried[s])
            part = [moved[:, b * head : (b + 1) * head] for b in range(blocks)]
            early = passes(split(part[0]), steps[s][1]) + part[1]
            late = passes(split(part[2]), steps[s][3]) + part[3]
            ab_ref[s, 1] = passes(split(early), tails[s]) + late

    def chain(s, half):
        return pltpu.make_async_remote_copy(
            src_ref=tx_ref.at[s, half],
            dst_ref=rx_ref.at[s, half],
            send_sem=send_x.at[s, half],
            recv_sem=recv_x.at[s, half],
            device_id=at(lax.rem(me + 1, count)),
            device_id_type=MESH,
        )

    def push(s):
        return pltpu.make_async_remote_copy(
            src_ref=ab_ref.at[s, 1],
            dst_ref=first_ref.at[s],
            send_sem=send_f.at[s],
            recv_sem=recv_f.at[s],
            device_id=at(last_one),
            device_id_type=MESH,
        )

    decoded = pltpu.make_async_remote_copy(
        src_ref=new_tx,
        dst_ref=new_rx,
        send_sem=send_n,
        recv_sem=recv_n,
        device_id=at(last_one),
        device_id_type=MESH,
    )

    def rows_to(s, k):
        to = lax.rem(me + k, count)
        return pltpu.make_async_remote_copy(
            src_ref=out_tx.at[s, to],
            dst_ref=out_rx.at[s],
            send_sem=send_o.at[s, k],
            recv_sem=recv_o.at[s],
            device_id=at(to),
            device_id_type=MESH,
        )

    @pl.when(in_chain)
    def _():
        pl.semaphore_wait(barrier, jnp.where(is_second, 2, 1))

    for s in range(seqs):

        @pl.when(is_second)
        def _():
            tx_ref[s, 0] = ab_ref[s, 0]

        @pl.when(me >= 2)
        def _():
            chain(s, 0).wait_recv()

        @pl.when(jnp.logical_and(in_chain, me >= 2))
        def _():
            tx_ref[s, 0] = product(rx_ref[s, 0], ab_ref[s, 0])

        @pl.when(in_chain)
        def _():
            if s:
                chain(s - 1, 0).wait_send()
            chain(s, 0).start()

    pushes()

    @pl.when(is_first)
    def _():
        pl.semaphore_wait(barrier, 1)
        for s in range(seqs):
            push(s).start()

    @pl.when(in_chain)
    def _():
        for s in range(seqs):

            @pl.when(is_second)
            def _():
                tx_ref[s, 1] = ab_ref[s, 1]

            @pl.when(jnp.logical_not(is_second))
            def _():
                chain(s, 1).wait_recv()
                tx_ref[s, 1] = product(rx_ref[s, 1], ab_ref[s, 0]) + ab_ref[s, 1]

            if s:
                chain(s - 1, 1).wait_send()
            else:
                chain(seqs - 1, 0).wait_send()
            chain(s, 1).start()

    @pl.when(is_second)
    def _():
        copies = [
            pltpu.make_async_copy(dec_hbm, dec_ref, load_sem.at[7]),
            pltpu.make_async_copy(wq_hbm, wq_ref, load_sem.at[8]),
        ]
        for copy in copies:
            copy.start()
        for copy in copies:
            copy.wait()
        dec = dec_ref[...]
        new_kv = silu(dot(dec, wkv_ref[...]))
        new_key = unit_rows(new_kv[:, :head])
        new_value = new_kv[:, head:]
        query = silu(dot(dec, wq_ref[...]))
        both = dot_nt(gate_ref[...], dec)
        row_n = iota((gates, seqs), 0)
        picked = [
            jnp.sum(jnp.where(row_n == head_index, part, 0.0), axis=0, keepdims=True)
            for part in (both[:gates], both[gates:])
        ]
        new_beta = jax.nn.sigmoid(picked[0] - write_offset)
        keep = jnp.exp(-rate * softplus(picked[1]))
        for s in range(seqs):
            one = slice(s, s + 1)
            new_tx[s, 0:1] = new_key[one]
            new_tx[s, 1:2] = query[one]
            new_tx[s, 2:3] = new_value[one]
            new_tx[s, 3:4] = jnp.broadcast_to(new_beta[:, one], (1, head))
            new_tx[s, 4:5] = jnp.broadcast_to(keep[:, one], (1, head))
            new_tx[s, 5:8] = jnp.zeros((3, head), F32)
        decoded.start()

    @pl.when(is_last)
    def _():
        pl.semaphore_wait(barrier, count - 1)
        load_r.wait()
        decoded.wait_recv()
        joins = []
        for s in range(seqs):
            push(s).wait_recv()
            joins.append(product(first_ref[s], rx_ref[s, 0]))
        for s in range(seqs):
            chain(s, 1).wait_recv()
            joined = joins[s] + rx_ref[s, 1]
            flipped = product(joined, ab_ref[s, 0]) + ab_ref[s, 1]
            new = new_rx[s]
            reads = product(new, flipped, dot_nt)
            final = jnp.transpose(flipped)
            key_read, query_read = reads[0:1], reads[1:2]
            value, beta, hold = new[2:3], new[3:4], new[4:5]
            inter = jnp.sum(new[0:1] * new[1:2], axis=-1, keepdims=True)
            key_col = jnp.transpose(new)[:, 0:1]
            cache = hold * final + key_col * (beta * value - (hold * beta) * key_read)
            mixed = hold * query_read - (hold * beta * inter) * key_read + (beta * inter) * value
            scale = lax.rsqrt(jnp.sum(mixed * mixed, axis=-1, keepdims=True) / head + epsilon)
            read = mixed * scale * gain_ref[...]
            each = head // count
            out_tx[s, :, :each] = cache.reshape(count, each, head)
            out_tx[s, :, each:] = jnp.broadcast_to(read.reshape(1, 1, head), (count, each, head))
            for k in range(1, count):
                rows_to(s, k).start()
            out_rx[s] = out_tx[s, last_one]

    for s in range(seqs):

        @pl.when(jnp.logical_not(is_last))
        def _():
            rows_to(s, 1).wait_recv()

        each = head // count
        cache_ref[s, 0] = out_rx[s, :each].astype(BF16)
        read_ref[s : s + 1] = out_rx[s, each : each + 1].astype(BF16)

    @pl.when(jnp.logical_not(is_last))
    def _():
        load_r.wait()

    @pl.when(is_first)
    def _():
        for s in range(seqs):
            push(s).wait_send()

    @pl.when(in_chain)
    def _():
        chain(seqs - 1, 1).wait_send()

    @pl.when(is_second)
    def _():
        decoded.wait_send()

    @pl.when(is_last)
    def _():
        for s in range(seqs):
            for k in range(1, count):
                rows_to(s, k).wait_send()


def per_device(
    tokens,
    decoded_input,
    query_weight,
    key_weight,
    value_weight,
    gate_weight,
    head_decay_rate,
    extra_log_decay,
    read_norm_gain,
):
    seqs, rows, width = tokens.shape
    head = key_weight.shape[1]
    count = lax.axis_size("sp")
    each = head // count
    gates = gate_weight.transpose(1, 2, 0).reshape(-1, width)
    vmem = pl.BlockSpec(memory_space=pltpu.VMEM)
    hbm = pl.BlockSpec(memory_space=pl.ANY)
    dma = pltpu.SemaphoreType.DMA
    return pl.pallas_call(
        functools.partial(kernel, seqs, rows, count),
        out_shape=(
            jax.ShapeDtypeStruct((seqs, 1, each, head), BF16),
            jax.ShapeDtypeStruct((seqs, head), BF16),
        ),
        in_specs=[hbm] * 9,
        out_specs=(vmem, vmem),
        scratch_shapes=[
            pltpu.VMEM((seqs, rows, width), BF16),
            pltpu.VMEM((seqs, width), BF16),
            pltpu.VMEM((width, 2 * head), BF16),
            pltpu.VMEM((width, head), BF16),
            pltpu.VMEM(gates.shape, BF16),
            pltpu.VMEM((1, 1), F32),
            pltpu.VMEM((seqs, 1, rows), F32),
            pltpu.VMEM((1, head), F32),
            pltpu.VMEM((seqs, rows, head), F32),
            pltpu.VMEM((seqs, rows, head), F32),
            pltpu.VMEM((seqs, 2, head, head), F32),
            pltpu.VMEM((seqs, 2, head, head), F32),
            pltpu.VMEM((seqs, 2, head, head), F32),
            pltpu.VMEM((seqs, head, head), F32),
            pltpu.VMEM((seqs, 8, head), F32),
            pltpu.VMEM((seqs, 8, head), F32),
            pltpu.VMEM((seqs, count, 2 * each, head), F32),
            pltpu.VMEM((seqs, 2 * each, head), F32),
            dma((8 + seqs,)),
            dma((seqs, 2)),
            dma((seqs, 2)),
            dma((seqs,)),
            dma((seqs,)),
            dma,
            dma,
            dma((seqs, count)),
            dma((seqs,)),
        ],
        compiler_params=pltpu.CompilerParams(collective_id=0, has_side_effects=True),
    )(
        tokens,
        decoded_input,
        query_weight,
        key_weight,
        value_weight,
        gates,
        head_decay_rate.reshape(1, 1),
        extra_log_decay,
        read_norm_gain.reshape(1, head),
    )


def solution(mesh):
    in_specs = (
        P("grp", "sp", None),
        P("grp", None),
        P(None, "tp"),
        P(None, "tp"),
        P(None, "tp"),
        P(),
        P("tp"),
        P("grp", "tp", "sp"),
        P(),
    )
    out_specs = (P("grp", "tp", "sp", None), P("grp", "tp"))
    return jax.shard_map(
        per_device, mesh=mesh, in_specs=in_specs, out_specs=out_specs, check_vma=False
    )
```

```python
import functools

import jax
import jax.numpy as jnp
from jax import lax
from jax.experimental import pallas as pl
from jax.experimental.pallas import tpu as pltpu
from jax.sharding import PartitionSpec as P

MESH = pl.DeviceIdType.MESH
F32 = jnp.float32
BF16 = jnp.bfloat16
epsilon = 1e-06
write_offset = 5.0
BLOCK = 64
GRANT = 60 * 1024 * 1024


def split(x):
    hi = x.astype(BF16)
    lo = (x - hi.astype(F32)).astype(BF16)
    return hi, lo


def dot(a, b):
    return jnp.dot(a, b, preferred_element_type=F32)


def dot_nt(a, b):
    return lax.dot_general(a, b, (((1,), (1,)), ((), ())), preferred_element_type=F32)


def passes(a, b, one=dot):
    return one(a[0], b[0]) + (one(a[0], b[1]) + one(a[1], b[0]))


def product(a, b, one=dot):
    return passes(split(a), split(b), one)


def silu(x):
    return x * jax.nn.sigmoid(x)


def softplus(x):
    return jnp.maximum(x, 0.0) + jnp.log1p(jnp.exp(-jnp.abs(x)))


def unit_rows(x):
    return x * lax.rsqrt(jnp.sum(x * x, axis=-1, keepdims=True) + epsilon)


def iota(shape, dim):
    return lax.broadcasted_iota(jnp.int32, shape, dim)


def kernel(
    seqs,
    rows,
    count,
    tok_hbm,
    dec_hbm,
    wq_hbm,
    wk_hbm,
    wv_hbm,
    gate_hbm,
    rate_hbm,
    extra_hbm,
    gain_hbm,
    cache_ref,
    read_ref,
    x_ref,
    dec_ref,
    wkv_ref,
    wq_ref,
    gate_ref,
    rate_ref,
    extra_ref,
    gain_ref,
    k_ref,
    v_ref,
    ab_ref,
    rx_ref,
    tx_ref,
    first_ref,
    new_tx,
    new_rx,
    out_tx,
    out_rx,
    load_sem,
    send_x,
    recv_x,
    send_f,
    recv_f,
    send_n,
    recv_n,
    send_o,
    recv_o,
):
    me = lax.axis_index("sp")
    head_index = lax.axis_index("tp")
    head = k_ref.shape[-1]
    gates = gate_ref.shape[0] // 2
    last_one = count - 1
    is_first = me == 0
    is_second = me == 1
    is_last = me == last_one
    in_chain = jnp.logical_and(me > 0, me < last_one)

    def load(source, target, place):
        copy = pltpu.make_async_copy(source, target, load_sem.at[place])
        copy.start()
        return copy

    load_w = [
        load(wk_hbm, wkv_ref.at[:, pl.ds(0, head)], 0),
        load(wv_hbm, wkv_ref.at[:, pl.ds(head, head)], 1),
    ]
    load_x = [load(tok_hbm.at[0], x_ref.at[0], 2)]
    load_g = [
        load(gate_hbm, gate_ref, 3),
        load(rate_hbm, rate_ref, 4),
        load(extra_hbm, extra_ref, 5),
    ]
    for s in range(1, seqs):
        load_x.append(load(tok_hbm.at[s], x_ref.at[s], 8 + s))
    load_r = load(gain_hbm, gain_ref, 6)

    def at(index):
        return {"sp": index}

    barrier = pltpu.get_barrier_semaphore()

    def greet(index):
        pl.semaphore_signal(barrier, inc=1, device_id=at(index), device_id_type=MESH)

    @pl.when(me >= 2)
    def _():
        greet(me - 1)

    @pl.when(is_last)
    def _():
        greet(0)

    @pl.when(jnp.logical_not(is_last))
    def _():
        greet(last_one)

    for copy in load_w:
        copy.wait()

    row_g = iota((gates, rows), 0)
    gate_rows = []
    for s in range(seqs):
        load_x[s].wait()
        kv = silu(dot(x_ref[s], wkv_ref[...]))
        k_ref[s] = unit_rows(kv[:, :head])
        v_ref[s] = kv[:, head:]
        if s == 0:
            for copy in load_g:
                copy.wait()
        both = dot_nt(gate_ref[...], x_ref[s])
        picked = [
            jnp.sum(jnp.where(row_g == head_index, part, 0.0), axis=0, keepdims=True)
            for part in (both[:gates], both[gates:])
        ]
        gate_rows.append(picked)
    rate = rate_ref[0]
    betas = [jax.nn.sigmoid(g[0] - write_offset) for g in gate_rows]
    decays = [-rate * softplus(g[1]) + extra_ref[s] for s, g in enumerate(gate_rows)]
    stacked = jnp.concatenate(decays, axis=0)
    hi, rest = split(stacked)
    rest32 = stacked - hi.astype(F32)
    lo = (rest32 - rest.astype(F32)).astype(BF16)
    parts = (hi, rest, lo)
    row_i = iota((rows, rows), 0)
    col_i = iota((rows, rows), 1)
    together = row_i // BLOCK == col_i // BLOCK
    upto = jnp.where(jnp.logical_and(together, row_i <= col_i), 1.0, 0.0).astype(BF16)
    whole = jnp.where(together, 1.0, 0.0).astype(BF16)
    running = sum(dot(part, upto) for part in parts)
    total = sum(dot(part, whole) for part in parts)
    grown = jnp.exp(running)
    packed = jnp.concatenate(
        betas
        + [running]
        + [betas[s] * grown[s : s + 1] for s in range(seqs)]
        + [jnp.exp(total - running)],
        axis=0,
    )
    columns = jnp.transpose(packed)

    def column(kind, s):
        place = kind * seqs + s
        return columns[:, place : place + 1]

    blocks = rows // BLOCK
    row_c = iota((BLOCK, rows), 0)
    lane_c = iota((BLOCK, rows), 1)
    inside = lax.bitwise_and(lane_c, BLOCK - 1)
    owner = lane_c // BLOCK
    own_lanes = [jnp.where(owner == b, 1.0, 0.0).astype(BF16) for b in range(blocks)]
    strict = row_c > inside
    eye = jnp.where(row_c == inside, 1.0, 0.0)

    def compact(full):
        out = jnp.where(owner == 0, full[:BLOCK], 0.0)
        for b in range(1, blocks):
            out = jnp.where(owner == b, full[b * BLOCK : (b + 1) * BLOCK], out)
        return out

    def diagonal(pair):
        return [jnp.concatenate([part * own for own in own_lanes], axis=0) for part in pair]

    n_mats, solves = [], []
    for s in range(seqs):
        halves = split(k_ref[s])
        inner = compact(passes(halves, halves, dot_nt))
        spread = compact(jnp.broadcast_to(column(1, s), (rows, rows))) - running[s : s + 1]
        below = jnp.where(strict, jnp.exp(jnp.where(strict, spread, 0.0)), 0.0)
        n_mat = compact(jnp.broadcast_to(column(0, s), (rows, rows))) * inner * below
        pair = row_c // 2 == inside // 2
        n_mats.append(n_mat)
        solves.append(eye - jnp.where(pair, n_mat, 0.0))
    depth = 1
    while 1 << depth < BLOCK:
        ri = lax.shift_right_logical(row_c, depth)
        ci = lax.shift_right_logical(inside, depth)
        mask = jnp.logical_and(ri == ci + 1, lax.bitwise_and(ci, 1) == 0)
        for s in range(seqs):
            t_mat = split(solves[s])
            inner = passes(split(jnp.where(mask, n_mats[s], 0.0)), diagonal(t_mat))
            solves[s] = solves[s] - passes(t_mat, diagonal(split(inner)))
        depth += 1

    head_eye = jnp.where(iota((head, head), 0) == iota((head, head), 1), 1.0, 0.0)
    row_b = iota((rows, 1), 0) // BLOCK
    inverse = [diagonal(split(t_mat)) for t_mat in solves]
    carried, steps = [], []
    for s in range(seqs):
        keys = k_ref[s]
        weights = passes(inverse[s], split(keys * column(2, s)))
        kept = keys * column(3, s)
        spans = jnp.concatenate(
            [jnp.where(row_b == b, kept, 0.0) for b in range(blocks)], axis=1
        )
        carried.append(split(spans))
        moved = passes(split(jnp.transpose(weights)), carried[s])
        step = []
        for b in range(blocks):
            decay = jnp.exp(total[s : s + 1, b * BLOCK : b * BLOCK + 1])
            step.append(split(decay * head_eye - moved[:, b * head : (b + 1) * head]))
        steps.append(step)
    tails = []
    for s in range(seqs):
        step = steps[s]
        tail = split(passes(step[2], step[3]))
        tails.append(tail)
        ab_ref[s, 0] = passes(split(passes(step[0], step[1])), tail)

    def pushes():
        for s in range(seqs):
            deltas = passes(inverse[s], split(v_ref[s] * column(0, s)))
            moved = passes(split(jnp.transpose(deltas)), carried[s])
            part = [moved[:, b * head : (b + 1) * head] for b in range(blocks)]
            early = passes(split(part[0]), steps[s][1]) + part[1]
            late = passes(split(part[2]), steps[s][3]) + part[3]
            ab_ref[s, 1] = passes(split(early), tails[s]) + late

    def chain(s, half):
        return pltpu.make_async_remote_copy(
            src_ref=tx_ref.at[s, half],
            dst_ref=rx_ref.at[s, half],
            send_sem=send_x.at[s, half],
            recv_sem=recv_x.at[s, half],
            device_id=at(lax.rem(me + 1, count)),
            device_id_type=MESH,
        )

    def push(s):
        return pltpu.make_async_remote_copy(
            src_ref=ab_ref.at[s, 1],
            dst_ref=first_ref.at[s],
            send_sem=send_f.at[s],
            recv_sem=recv_f.at[s],
            device_id=at(last_one),
            device_id_type=MESH,
        )

    decoded = pltpu.make_async_remote_copy(
        src_ref=new_tx,
        dst_ref=new_rx,
        send_sem=send_n,
        recv_sem=recv_n,
        device_id=at(last_one),
        device_id_type=MESH,
    )

    def rows_to(s, k):
        to = lax.rem(me + k, count)
        return pltpu.make_async_remote_copy(
            src_ref=out_tx.at[s, to],
            dst_ref=out_rx.at[s],
            send_sem=send_o.at[s, k],
            recv_sem=recv_o.at[s],
            device_id=at(to),
            device_id_type=MESH,
        )

    @pl.when(in_chain)
    def _():
        pl.semaphore_wait(barrier, 1)

    for s in range(seqs):

        @pl.when(is_second)
        def _():
            tx_ref[s, 0] = ab_ref[s, 0]

        @pl.when(me >= 2)
        def _():
            chain(s, 0).wait_recv()

        @pl.when(jnp.logical_and(in_chain, me >= 2))
        def _():
            tx_ref[s, 0] = product(rx_ref[s, 0], ab_ref[s, 0])

        @pl.when(in_chain)
        def _():
            if s:
                chain(s - 1, 0).wait_send()
            chain(s, 0).start()

    pushes()

    @pl.when(is_first)
    def _():
        pl.semaphore_wait(barrier, 1)
        for s in range(seqs):
            push(s).start()
        copies = [
            pltpu.make_async_copy(dec_hbm, dec_ref, load_sem.at[7]),
            pltpu.make_async_copy(wq_hbm, wq_ref, load_sem.at[8]),
        ]
        for copy in copies:
            copy.start()
        for copy in copies:
            copy.wait()
        dec = dec_ref[...]
        new_kv = silu(dot(dec, wkv_ref[...]))
        new_key = unit_rows(new_kv[:, :head])
        new_value = new_kv[:, head:]
        query = silu(dot(dec, wq_ref[...]))
        both = dot_nt(gate_ref[...], dec)
        row_n = iota((gates, seqs), 0)
        picked = [
            jnp.sum(jnp.where(row_n == head_index, part, 0.0), axis=0, keepdims=True)
            for part in (both[:gates], both[gates:])
        ]
        new_beta = jax.nn.sigmoid(picked[0] - write_offset)
        keep = jnp.exp(-rate * softplus(picked[1]))
        for s in range(seqs):
            one = slice(s, s + 1)
            new_tx[s, 0:1] = new_key[one]
            new_tx[s, 1:2] = query[one]
            new_tx[s, 2:3] = new_value[one]
            new_tx[s, 3:4] = jnp.broadcast_to(new_beta[:, one], (1, head))
            new_tx[s, 4:5] = jnp.broadcast_to(keep[:, one], (1, head))
            new_tx[s, 5:8] = jnp.zeros((3, head), F32)
        decoded.start()

    @pl.when(in_chain)
    def _():
        for s in range(seqs):

            @pl.when(is_second)
            def _():
                tx_ref[s, 1] = ab_ref[s, 1]

            @pl.when(jnp.logical_not(is_second))
            def _():
                chain(s, 1).wait_recv()
                tx_ref[s, 1] = product(rx_ref[s, 1], ab_ref[s, 0]) + ab_ref[s, 1]

            if s:
                chain(s - 1, 1).wait_send()
            else:
                chain(seqs - 1, 0).wait_send()
            chain(s, 1).start()

    @pl.when(is_last)
    def _():
        pl.semaphore_wait(barrier, count - 1)
        load_r.wait()
        decoded.wait_recv()
        joins = []
        for s in range(seqs):
            push(s).wait_recv()
            joins.append(product(first_ref[s], rx_ref[s, 0]))
        for s in range(seqs):
            chain(s, 1).wait_recv()
            joined = joins[s] + rx_ref[s, 1]
            flipped = product(joined, ab_ref[s, 0]) + ab_ref[s, 1]
            new = new_rx[s]
            reads = product(new, flipped, dot_nt)
            final = jnp.transpose(flipped)
            key_read, query_read = reads[0:1], reads[1:2]
            value, beta, hold = new[2:3], new[3:4], new[4:5]
            inter = jnp.sum(new[0:1] * new[1:2], axis=-1, keepdims=True)
            key_col = jnp.transpose(new)[:, 0:1]
            cache = hold * final + key_col * (beta * value - (hold * beta) * key_read)
            mixed = hold * query_read - (hold * beta * inter) * key_read + (beta * inter) * value
            scale = lax.rsqrt(jnp.sum(mixed * mixed, axis=-1, keepdims=True) / head + epsilon)
            read = mixed * scale * gain_ref[...]
            each = head // count
            out_tx[s, :, :each] = cache.reshape(count, each, head)
            out_tx[s, :, each:] = jnp.broadcast_to(read.reshape(1, 1, head), (count, each, head))
            for k in range(1, count):
                rows_to(s, k).start()
            out_rx[s] = out_tx[s, last_one]

    for s in range(seqs):

        @pl.when(jnp.logical_not(is_last))
        def _():
            rows_to(s, 1).wait_recv()

        each = head // count
        cache_ref[s, 0] = out_rx[s, :each].astype(BF16)
        read_ref[s : s + 1] = out_rx[s, each : each + 1].astype(BF16)

    @pl.when(jnp.logical_not(is_last))
    def _():
        load_r.wait()

    @pl.when(is_first)
    def _():
        for s in range(seqs):
            push(s).wait_send()
        decoded.wait_send()

    @pl.when(in_chain)
    def _():
        chain(seqs - 1, 1).wait_send()

    @pl.when(is_last)
    def _():
        for s in range(seqs):
            for k in range(1, count):
                rows_to(s, k).wait_send()


def per_device(
    tokens,
    decoded_input,
    query_weight,
    key_weight,
    value_weight,
    gate_weight,
    head_decay_rate,
    extra_log_decay,
    read_norm_gain,
):
    seqs, rows, width = tokens.shape
    head = key_weight.shape[1]
    count = lax.axis_size("sp")
    each = head // count
    gates = gate_weight.transpose(1, 2, 0).reshape(-1, width)
    vmem = pl.BlockSpec(memory_space=pltpu.VMEM)
    hbm = pl.BlockSpec(memory_space=pltpu.HBM)
    dma = pltpu.SemaphoreType.DMA
    return pl.pallas_call(
        functools.partial(kernel, seqs, rows, count),
        out_shape=(
            jax.ShapeDtypeStruct((seqs, 1, each, head), BF16),
            jax.ShapeDtypeStruct((seqs, head), BF16),
        ),
        in_specs=[hbm] * 9,
        out_specs=(vmem, vmem),
        scratch_shapes=[
            pltpu.VMEM((seqs, rows, width), BF16),
            pltpu.VMEM((seqs, width), BF16),
            pltpu.VMEM((width, 2 * head), BF16),
            pltpu.VMEM((width, head), BF16),
            pltpu.VMEM(gates.shape, BF16),
            pltpu.SMEM((1,), F32),
            pltpu.VMEM((seqs, 1, rows), F32),
            pltpu.VMEM((1, head), F32),
            pltpu.VMEM((seqs, rows, head), F32),
            pltpu.VMEM((seqs, rows, head), F32),
            pltpu.VMEM((seqs, 2, head, head), F32),
            pltpu.VMEM((seqs, 2, head, head), F32),
            pltpu.VMEM((seqs, 2, head, head), F32),
            pltpu.VMEM((seqs, head, head), F32),
            pltpu.VMEM((seqs, 8, head), F32),
            pltpu.VMEM((seqs, 8, head), F32),
            pltpu.VMEM((seqs, count, 2 * each, head), F32),
            pltpu.VMEM((seqs, 2 * each, head), F32),
            dma((8 + seqs,)),
            dma((seqs, 2)),
            dma((seqs, 2)),
            dma((seqs,)),
            dma((seqs,)),
            dma,
            dma,
            dma((seqs, count)),
            dma((seqs,)),
        ],
        compiler_params=pltpu.CompilerParams(
            collective_id=0, has_side_effects=True, vmem_limit_bytes=GRANT
        ),
    )(
        tokens,
        decoded_input,
        query_weight,
        key_weight,
        value_weight,
        gates,
        head_decay_rate,
        extra_log_decay,
        read_norm_gain.reshape(1, head),
    )


def solution(mesh):
    in_specs = (
        P("grp", "sp", None),
        P("grp", None),
        P(None, "tp"),
        P(None, "tp"),
        P(None, "tp"),
        P(),
        P("tp"),
        P("grp", "tp", "sp"),
        P(),
    )
    out_specs = (P("grp", "tp", "sp", None), P("grp", "tp"))
    return jax.shard_map(
        per_device, mesh=mesh, in_specs=in_specs, out_specs=out_specs, check_vma=False
    )
```

```python
import functools

import jax
import jax.numpy as jnp
from jax import lax
from jax.experimental import pallas as pl
from jax.experimental.pallas import tpu as pltpu
from jax.sharding import PartitionSpec as P

MESH = pl.DeviceIdType.MESH
F32 = jnp.float32
BF16 = jnp.bfloat16
epsilon = 1e-06
write_offset = 5.0
BLOCK = 64
CHUNKS = 4
GRANT = 60 * 1024 * 1024


def split(x):
    hi = x.astype(BF16)
    lo = (x - hi.astype(F32)).astype(BF16)
    return hi, lo


def dot(a, b):
    return jnp.dot(a, b, preferred_element_type=F32)


def dot_nt(a, b):
    return lax.dot_general(a, b, (((1,), (1,)), ((), ())), preferred_element_type=F32)


def passes(a, b, one=dot):
    return one(a[0], b[0]) + (one(a[0], b[1]) + one(a[1], b[0]))


def product(a, b, one=dot):
    return passes(split(a), split(b), one)


def silu(x):
    return x * jax.nn.sigmoid(x)


def softplus(x):
    return jnp.maximum(x, 0.0) + jnp.log1p(jnp.exp(-jnp.abs(x)))


def unit_rows(x):
    return x * lax.rsqrt(jnp.sum(x * x, axis=-1, keepdims=True) + epsilon)


def iota(shape, dim):
    return lax.broadcasted_iota(jnp.int32, shape, dim)


def kernel(
    seqs,
    rows,
    count,
    tok_hbm,
    dec_hbm,
    wq_hbm,
    wk_hbm,
    wv_hbm,
    gate_hbm,
    rate_hbm,
    extra_hbm,
    gain_hbm,
    cache_ref,
    read_ref,
    x_ref,
    dec_ref,
    wkv_ref,
    wq_ref,
    gate_ref,
    rate_ref,
    extra_ref,
    gain_ref,
    k_ref,
    v_ref,
    ab_ref,
    rx_ref,
    tx_ref,
    first_ref,
    new_tx,
    new_rx,
    out_tx,
    out_rx,
    load_sem,
    send_x,
    recv_x,
    send_f,
    recv_f,
    send_n,
    recv_n,
    send_o,
    recv_o,
):
    me = lax.axis_index("sp")
    head_index = lax.axis_index("tp")
    head = k_ref.shape[-1]
    gates = gate_ref.shape[0] // 2
    last_one = count - 1
    is_first = me == 0
    is_second = me == 1
    is_last = me == last_one
    in_chain = jnp.logical_and(me > 0, me < last_one)

    def load(source, target, place):
        copy = pltpu.make_async_copy(source, target, load_sem.at[place])
        copy.start()
        return copy

    width = x_ref.shape[-1]
    wide = width // CHUNKS
    loads = []
    for c in range(CHUNKS):
        cut = pl.ds(c * wide, wide)
        pairs = [
            (wk_hbm.at[cut], wkv_ref.at[cut, pl.ds(0, head)]),
            (wv_hbm.at[cut], wkv_ref.at[cut, pl.ds(head, head)]),
        ]
        pairs += [(tok_hbm.at[s, :, cut], x_ref.at[s, :, cut]) for s in range(seqs)]
        pairs.append((gate_hbm.at[:, cut], gate_ref.at[:, cut]))
        loads.append(
            [load(pair[0], pair[1], 8 + c * len(pairs) + i) for i, pair in enumerate(pairs)]
        )
    load_g = [load(rate_hbm, rate_ref, 4), load(extra_hbm, extra_ref, 5)]
    load_r = load(gain_hbm, gain_ref, 6)

    def at(index):
        return {"sp": index}

    barrier = pltpu.get_barrier_semaphore()

    def greet(index):
        pl.semaphore_signal(barrier, inc=1, device_id=at(index), device_id_type=MESH)

    @pl.when(me >= 2)
    def _():
        greet(me - 1)

    @pl.when(is_last)
    def _():
        greet(0)

    @pl.when(jnp.logical_not(is_last))
    def _():
        greet(last_one)

    row_g = iota((gates, rows), 0)
    sums = [None] * seqs
    gate_sums = [None] * seqs
    for c in range(CHUNKS):
        for copy in loads[c]:
            copy.wait()
        cut = slice(c * wide, (c + 1) * wide)
        for s in range(seqs):
            part = dot(x_ref[s, :, cut], wkv_ref[cut])
            sums[s] = part if c == 0 else sums[s] + part
            part = dot_nt(gate_ref[:, cut], x_ref[s, :, cut])
            gate_sums[s] = part if c == 0 else gate_sums[s] + part
    for copy in load_g:
        copy.wait()
    gate_rows = []
    for s in range(seqs):
        kv = silu(sums[s])
        k_ref[s] = unit_rows(kv[:, :head])
        v_ref[s] = kv[:, head:]
        picked = [
            jnp.sum(jnp.where(row_g == head_index, part, 0.0), axis=0, keepdims=True)
            for part in (gate_sums[s][:gates], gate_sums[s][gates:])
        ]
        gate_rows.append(picked)
    rate = rate_ref[0]
    betas = [jax.nn.sigmoid(g[0] - write_offset) for g in gate_rows]
    decays = [-rate * softplus(g[1]) + extra_ref[s] for s, g in enumerate(gate_rows)]
    stacked = jnp.concatenate(decays, axis=0)
    hi, rest = split(stacked)
    rest32 = stacked - hi.astype(F32)
    lo = (rest32 - rest.astype(F32)).astype(BF16)
    parts = (hi, rest, lo)
    row_i = iota((rows, rows), 0)
    col_i = iota((rows, rows), 1)
    together = row_i // BLOCK == col_i // BLOCK
    upto = jnp.where(jnp.logical_and(together, row_i <= col_i), 1.0, 0.0).astype(BF16)
    whole = jnp.where(together, 1.0, 0.0).astype(BF16)
    running = sum(dot(part, upto) for part in parts)
    total = sum(dot(part, whole) for part in parts)
    grown = jnp.exp(running)
    packed = jnp.concatenate(
        betas
        + [running]
        + [betas[s] * grown[s : s + 1] for s in range(seqs)]
        + [jnp.exp(total - running)],
        axis=0,
    )
    columns = jnp.transpose(packed)

    def column(kind, s):
        place = kind * seqs + s
        return columns[:, place : place + 1]

    blocks = rows // BLOCK
    row_c = iota((BLOCK, rows), 0)
    lane_c = iota((BLOCK, rows), 1)
    inside = lax.bitwise_and(lane_c, BLOCK - 1)
    owner = lane_c // BLOCK
    own_lanes = [jnp.where(owner == b, 1.0, 0.0).astype(BF16) for b in range(blocks)]
    strict = row_c > inside
    eye = jnp.where(row_c == inside, 1.0, 0.0)

    def compact(full):
        out = jnp.where(owner == 0, full[:BLOCK], 0.0)
        for b in range(1, blocks):
            out = jnp.where(owner == b, full[b * BLOCK : (b + 1) * BLOCK], out)
        return out

    def diagonal(pair):
        return [jnp.concatenate([part * own for own in own_lanes], axis=0) for part in pair]

    n_mats, solves = [], []
    for s in range(seqs):
        halves = split(k_ref[s])
        inner = compact(passes(halves, halves, dot_nt))
        spread = compact(jnp.broadcast_to(column(1, s), (rows, rows))) - running[s : s + 1]
        below = jnp.where(strict, jnp.exp(jnp.where(strict, spread, 0.0)), 0.0)
        n_mat = compact(jnp.broadcast_to(column(0, s), (rows, rows))) * inner * below
        pair = row_c // 2 == inside // 2
        n_mats.append(n_mat)
        solves.append(eye - jnp.where(pair, n_mat, 0.0))
    depth = 1
    while 1 << depth < BLOCK:
        ri = lax.shift_right_logical(row_c, depth)
        ci = lax.shift_right_logical(inside, depth)
        mask = jnp.logical_and(ri == ci + 1, lax.bitwise_and(ci, 1) == 0)
        for s in range(seqs):
            t_mat = split(solves[s])
            inner = passes(split(jnp.where(mask, n_mats[s], 0.0)), diagonal(t_mat))
            solves[s] = solves[s] - passes(t_mat, diagonal(split(inner)))
        depth += 1

    head_eye = jnp.where(iota((head, head), 0) == iota((head, head), 1), 1.0, 0.0)
    row_b = iota((rows, 1), 0) // BLOCK
    inverse = [diagonal(split(t_mat)) for t_mat in solves]
    pieces = []
    for s in range(seqs):
        keys = k_ref[s]
        right = jnp.concatenate([keys * column(2, s), v_ref[s] * column(0, s)], axis=1)
        solved = passes(inverse[s], split(right))
        kept = keys * column(3, s)
        spans = jnp.concatenate(
            [jnp.where(row_b == b, kept, 0.0) for b in range(blocks)], axis=1
        )
        moved = passes(split(jnp.transpose(solved)), split(spans))
        piece = []
        for b in range(blocks):
            decay = jnp.exp(total[s : s + 1, b * BLOCK : b * BLOCK + 1])
            part = moved[:, b * head : (b + 1) * head]
            piece.append((decay * head_eye - part[:head], part[head:]))
        pieces.append(piece)
    while len(pieces[0]) > 1:
        for s in range(seqs):
            merged = []
            for early, late in zip(pieces[s][0::2], pieces[s][1::2]):
                both = product(jnp.concatenate(early, axis=0), late[0])
                merged.append((both[:head], both[head:] + late[1]))
            pieces[s] = merged
    for s in range(seqs):
        ab_ref[s, 0], ab_ref[s, 1] = pieces[s][0]

    def chain(s, half):
        return pltpu.make_async_remote_copy(
            src_ref=tx_ref.at[s, half],
            dst_ref=rx_ref.at[s, half],
            send_sem=send_x.at[s, half],
            recv_sem=recv_x.at[s, half],
            device_id=at(lax.rem(me + 1, count)),
            device_id_type=MESH,
        )

    def push(s):
        return pltpu.make_async_remote_copy(
            src_ref=ab_ref.at[s, 1],
            dst_ref=first_ref.at[s],
            send_sem=send_f.at[s],
            recv_sem=recv_f.at[s],
            device_id=at(last_one),
            device_id_type=MESH,
        )

    decoded = pltpu.make_async_remote_copy(
        src_ref=new_tx,
        dst_ref=new_rx,
        send_sem=send_n,
        recv_sem=recv_n,
        device_id=at(last_one),
        device_id_type=MESH,
    )

    def rows_to(s, k):
        to = lax.rem(me + k, count)
        return pltpu.make_async_remote_copy(
            src_ref=out_tx.at[s, to],
            dst_ref=out_rx.at[s],
            send_sem=send_o.at[s, k],
            recv_sem=recv_o.at[s],
            device_id=at(to),
            device_id_type=MESH,
        )

    @pl.when(is_first)
    def _():
        pl.semaphore_wait(barrier, 1)
        for s in range(seqs):
            push(s).start()
        copies = [
            pltpu.make_async_copy(dec_hbm, dec_ref, load_sem.at[7]),
            pltpu.make_async_copy(wq_hbm, wq_ref, load_sem.at[3]),
        ]
        for copy in copies:
            copy.start()
        for copy in copies:
            copy.wait()
        dec = dec_ref[...]
        new_kv = silu(dot(dec, wkv_ref[...]))
        new_key = unit_rows(new_kv[:, :head])
        new_value = new_kv[:, head:]
        query = silu(dot(dec, wq_ref[...]))
        both = dot_nt(gate_ref[...], dec)
        row_n = iota((gates, seqs), 0)
        picked = [
            jnp.sum(jnp.where(row_n == head_index, part, 0.0), axis=0, keepdims=True)
            for part in (both[:gates], both[gates:])
        ]
        new_beta = jax.nn.sigmoid(picked[0] - write_offset)
        keep = jnp.exp(-rate * softplus(picked[1]))
        for s in range(seqs):
            one = slice(s, s + 1)
            new_tx[s, 0:1] = new_key[one]
            new_tx[s, 1:2] = query[one]
            new_tx[s, 2:3] = new_value[one]
            new_tx[s, 3:4] = jnp.broadcast_to(new_beta[:, one], (1, head))
            new_tx[s, 4:5] = jnp.broadcast_to(keep[:, one], (1, head))
            new_tx[s, 5:8] = jnp.zeros((3, head), F32)
        decoded.start()

    @pl.when(in_chain)
    def _():
        pl.semaphore_wait(barrier, 1)
        for half in range(2):
            for s in range(seqs):

                @pl.when(is_second)
                def _():
                    tx_ref[s, half] = ab_ref[s, half]

                @pl.when(jnp.logical_not(is_second))
                def _():
                    chain(s, half).wait_recv()
                    moved = product(rx_ref[s, half], ab_ref[s, 0])
                    tx_ref[s, half] = moved + ab_ref[s, 1] if half else moved

                chain(s, half).start()

    @pl.when(is_last)
    def _():
        pl.semaphore_wait(barrier, count - 1)
        load_r.wait()
        decoded.wait_recv()
        ahead = []
        for s in range(seqs):
            step, own = split(ab_ref[s, 0]), ab_ref[s, 1]
            new = split(new_rx[s])
            read_step = passes(new, step, dot_nt)
            ahead.append((step, split(read_step), passes(new, split(own), dot_nt)))
        joins = []
        for s in range(seqs):
            chain(s, 0).wait_recv()
            push(s).wait_recv()
            joins.append(product(first_ref[s], rx_ref[s, 0]))
        for s in range(seqs):
            step, read_step, read_own = ahead[s]
            chain(s, 1).wait_recv()
            joined = split(joins[s] + rx_ref[s, 1])
            flipped = passes(joined, step) + ab_ref[s, 1]
            reads = passes(read_step, joined, dot_nt) + read_own
            new = new_rx[s]
            final = jnp.transpose(flipped)
            key_read, query_read = reads[0:1], reads[1:2]
            value, beta, hold = new[2:3], new[3:4], new[4:5]
            inter = jnp.sum(new[0:1] * new[1:2], axis=-1, keepdims=True)
            key_col = jnp.transpose(new)[:, 0:1]
            cache = hold * final + key_col * (beta * value - (hold * beta) * key_read)
            mixed = hold * query_read - (hold * beta * inter) * key_read + (beta * inter) * value
            scale = lax.rsqrt(jnp.sum(mixed * mixed, axis=-1, keepdims=True) / head + epsilon)
            read = mixed * scale * gain_ref[...]
            each = head // count
            out_tx[s, :, :each] = cache.reshape(count, each, head)
            out_tx[s, :, each:] = jnp.broadcast_to(read.reshape(1, 1, head), (count, each, head))
            for k in range(1, count):
                rows_to(s, k).start()
            out_rx[s] = out_tx[s, last_one]

    for s in range(seqs):

        @pl.when(jnp.logical_not(is_last))
        def _():
            rows_to(s, 1).wait_recv()

        each = head // count
        cache_ref[s, 0] = out_rx[s, :each].astype(BF16)
        read_ref[s : s + 1] = out_rx[s, each : each + 1].astype(BF16)

    @pl.when(jnp.logical_not(is_last))
    def _():
        load_r.wait()

    @pl.when(is_first)
    def _():
        for s in range(seqs):
            push(s).wait_send()
        decoded.wait_send()

    @pl.when(in_chain)
    def _():
        for half in range(2):
            for s in range(seqs):
                chain(s, half).wait_send()

    @pl.when(is_last)
    def _():
        for s in range(seqs):
            for k in range(1, count):
                rows_to(s, k).wait_send()


def per_device(
    tokens,
    decoded_input,
    query_weight,
    key_weight,
    value_weight,
    gate_weight,
    head_decay_rate,
    extra_log_decay,
    read_norm_gain,
):
    seqs, rows, width = tokens.shape
    head = key_weight.shape[1]
    count = lax.axis_size("sp")
    each = head // count
    gates = gate_weight.transpose(1, 2, 0).reshape(-1, width)
    vmem = pl.BlockSpec(memory_space=pltpu.VMEM)
    hbm = pl.BlockSpec(memory_space=pltpu.HBM)
    dma = pltpu.SemaphoreType.DMA
    return pl.pallas_call(
        functools.partial(kernel, seqs, rows, count),
        out_shape=(
            jax.ShapeDtypeStruct((seqs, 1, each, head), BF16),
            jax.ShapeDtypeStruct((seqs, head), BF16),
        ),
        in_specs=[hbm] * 9,
        out_specs=(vmem, vmem),
        scratch_shapes=[
            pltpu.VMEM((seqs, rows, width), BF16),
            pltpu.VMEM((seqs, width), BF16),
            pltpu.VMEM((width, 2 * head), BF16),
            pltpu.VMEM((width, head), BF16),
            pltpu.VMEM(gates.shape, BF16),
            pltpu.SMEM((1,), F32),
            pltpu.VMEM((seqs, 1, rows), F32),
            pltpu.VMEM((1, head), F32),
            pltpu.VMEM((seqs, rows, head), F32),
            pltpu.VMEM((seqs, rows, head), F32),
            pltpu.VMEM((seqs, 2, head, head), F32),
            pltpu.VMEM((seqs, 2, head, head), F32),
            pltpu.VMEM((seqs, 2, head, head), F32),
            pltpu.VMEM((seqs, head, head), F32),
            pltpu.VMEM((seqs, 8, head), F32),
            pltpu.VMEM((seqs, 8, head), F32),
            pltpu.VMEM((seqs, count, 2 * each, head), F32),
            pltpu.VMEM((seqs, 2 * each, head), F32),
            dma((8 + CHUNKS * (seqs + 3),)),
            dma((seqs, 2)),
            dma((seqs, 2)),
            dma((seqs,)),
            dma((seqs,)),
            dma,
            dma,
            dma((seqs, count)),
            dma((seqs,)),
        ],
        compiler_params=pltpu.CompilerParams(
            collective_id=0, has_side_effects=True, vmem_limit_bytes=GRANT
        ),
    )(
        tokens,
        decoded_input,
        query_weight,
        key_weight,
        value_weight,
        gates,
        head_decay_rate,
        extra_log_decay,
        read_norm_gain.reshape(1, head),
    )


def solution(mesh):
    in_specs = (
        P("grp", "sp", None),
        P("grp", None),
        P(None, "tp"),
        P(None, "tp"),
        P(None, "tp"),
        P(),
        P("tp"),
        P("grp", "tp", "sp"),
        P(),
    )
    out_specs = (P("grp", "tp", "sp", None), P("grp", "tp"))
    return jax.shard_map(
        per_device, mesh=mesh, in_specs=in_specs, out_specs=out_specs, check_vma=False
    )
```

```python
import functools

import jax
import jax.numpy as jnp
from jax import lax
from jax.experimental import pallas as pl
from jax.experimental.pallas import tpu as pltpu
from jax.sharding import PartitionSpec as P

MESH = pl.DeviceIdType.MESH
F32 = jnp.float32
BF16 = jnp.bfloat16
epsilon = 1e-06
write_offset = 5.0
BLOCK = 64
CHUNKS = 4
GROUP = 8
GRANT = 24 << 20


def split(x):
    hi = x.astype(BF16)
    lo = (x - hi.astype(F32)).astype(BF16)
    return hi, lo


def dot(a, b):
    return jnp.dot(a, b, preferred_element_type=F32)


def dot_nt(a, b):
    return lax.dot_general(a, b, (((1,), (1,)), ((), ())), preferred_element_type=F32)


def passes(a, b, one=dot):
    return one(a[0], b[0]) + (one(a[0], b[1]) + one(a[1], b[0]))


def product(a, b, one=dot):
    return passes(split(a), split(b), one)


def silu(x):
    return x * jax.nn.sigmoid(x)


def softplus(x):
    return jnp.maximum(x, 0.0) + jnp.log1p(jnp.exp(-jnp.abs(x)))


def unit_rows(x):
    return x * lax.rsqrt(jnp.sum(x * x, axis=-1, keepdims=True) + epsilon)


def iota(shape, dim):
    return lax.broadcasted_iota(jnp.int32, shape, dim)


def kernel(
    seqs,
    rows,
    count,
    tok_hbm,
    dec_hbm,
    wq_hbm,
    wk_hbm,
    wv_hbm,
    gate_hbm,
    rate_hbm,
    extra_hbm,
    gain_hbm,
    cache_ref,
    read_ref,
    x_ref,
    dec_ref,
    wkv_ref,
    wq_ref,
    gate_ref,
    rate_ref,
    extra_ref,
    gain_ref,
    k_ref,
    v_ref,
    ab_ref,
    rx_ref,
    tx_ref,
    first_ref,
    new_tx,
    new_rx,
    out_tx,
    out_rx,
    load_sem,
    send_x,
    recv_x,
    send_f,
    recv_f,
    send_n,
    recv_n,
    send_o,
    recv_o,
):
    me = lax.axis_index("sp")
    head_index = lax.axis_index("tp")
    head = k_ref.shape[-1]
    gates = GROUP
    heads = gate_hbm.shape[0] // 2
    first = pl.multiple_of(head_index // GROUP * GROUP, GROUP)
    local_head = lax.rem(head_index, GROUP)
    last_one = count - 1
    is_first = me == 0
    is_second = me == 1
    is_decoder = me == last_one - 1
    is_last = me == last_one
    in_chain = jnp.logical_and(me > 0, me < last_one)

    def load(source, target, place):
        copy = pltpu.make_async_copy(source, target, load_sem.at[place])
        copy.start()
        return copy

    width = x_ref.shape[-1]
    wide = width // CHUNKS
    loads = []
    for c in range(CHUNKS):
        cut = pl.ds(c * wide, wide)
        pairs = [
            (wk_hbm.at[cut], wkv_ref.at[cut, pl.ds(0, head)]),
            (wv_hbm.at[cut], wkv_ref.at[cut, pl.ds(head, head)]),
        ]
        pairs += [(tok_hbm.at[s, :, cut], x_ref.at[s, :, cut]) for s in range(seqs)]
        pairs += [
            (gate_hbm.at[pl.ds(first + g // GROUP * heads, GROUP), cut], gate_ref.at[pl.ds(g, GROUP), cut])
            for g in (0, GROUP)
        ]
        loads.append(
            [load(pair[0], pair[1], 8 + c * len(pairs) + i) for i, pair in enumerate(pairs)]
        )
    load_g = [load(rate_hbm, rate_ref, 4), load(extra_hbm, extra_ref, 5)]
    load_r = load(gain_hbm, gain_ref, 6)
    load_dec = [
        pltpu.make_async_copy(dec_hbm, dec_ref, load_sem.at[7]),
        pltpu.make_async_copy(wq_hbm, wq_ref, load_sem.at[3]),
    ]

    @pl.when(is_decoder)
    def _():
        for copy in load_dec:
            copy.start()


    def at(index):
        return {"sp": index}

    barrier = pltpu.get_barrier_semaphore()

    def greet(index):
        pl.semaphore_signal(barrier, inc=1, device_id=at(index), device_id_type=MESH)

    @pl.when(me >= 2)
    def _():
        greet(me - 1)

    @pl.when(is_last)
    def _():
        greet(0)

    @pl.when(jnp.logical_not(is_last))
    def _():
        greet(last_one)

    row_g = iota((gates, rows), 0)
    sums = [None] * seqs
    gate_sums = [None] * seqs
    for c in range(CHUNKS):
        for copy in loads[c]:
            copy.wait()
        cut = slice(c * wide, (c + 1) * wide)
        for s in range(seqs):
            part = dot(x_ref[s, :, cut], wkv_ref[cut])
            sums[s] = part if c == 0 else sums[s] + part
            part = dot_nt(gate_ref[:, cut], x_ref[s, :, cut])
            gate_sums[s] = part if c == 0 else gate_sums[s] + part
    for copy in load_g:
        copy.wait()
    gate_rows = []
    for s in range(seqs):
        kv = silu(sums[s])
        k_ref[s] = unit_rows(kv[:, :head])
        v_ref[s] = kv[:, head:]
        picked = [
            jnp.sum(jnp.where(row_g == local_head, part, 0.0), axis=0, keepdims=True)
            for part in (gate_sums[s][:gates], gate_sums[s][gates:])
        ]
        gate_rows.append(picked)
    rate = rate_ref[0]
    betas = [jax.nn.sigmoid(g[0] - write_offset) for g in gate_rows]
    decays = [-rate * softplus(g[1]) + extra_ref[s] for s, g in enumerate(gate_rows)]
    stacked = jnp.concatenate(decays, axis=0)
    hi, rest = split(stacked)
    rest32 = stacked - hi.astype(F32)
    lo = (rest32 - rest.astype(F32)).astype(BF16)
    parts = (hi, rest, lo)
    row_i = iota((rows, rows), 0)
    col_i = iota((rows, rows), 1)
    together = row_i // BLOCK == col_i // BLOCK
    upto = jnp.where(jnp.logical_and(together, row_i <= col_i), 1.0, 0.0).astype(BF16)
    whole = jnp.where(together, 1.0, 0.0).astype(BF16)
    running = sum(dot(part, upto) for part in parts)
    total = sum(dot(part, whole) for part in parts)
    grown = jnp.exp(running)
    packed = jnp.concatenate(
        betas
        + [running]
        + [betas[s] * grown[s : s + 1] for s in range(seqs)]
        + [jnp.exp(total - running)],
        axis=0,
    )
    columns = jnp.transpose(packed)

    def column(kind, s):
        place = kind * seqs + s
        return columns[:, place : place + 1]

    blocks = rows // BLOCK
    row_c = iota((BLOCK, rows), 0)
    lane_c = iota((BLOCK, rows), 1)
    inside = lax.bitwise_and(lane_c, BLOCK - 1)
    owner = lane_c // BLOCK
    own_lanes = [jnp.where(owner == b, 1.0, 0.0).astype(BF16) for b in range(blocks)]
    strict = row_c > inside
    eye = jnp.where(row_c == inside, 1.0, 0.0)

    def compact(full):
        out = jnp.where(owner == 0, full[:BLOCK], 0.0)
        for b in range(1, blocks):
            out = jnp.where(owner == b, full[b * BLOCK : (b + 1) * BLOCK], out)
        return out

    def diagonal(pair):
        return [jnp.concatenate([part * own for own in own_lanes], axis=0) for part in pair]

    n_mats, solves = [], []
    for s in range(seqs):
        halves = split(k_ref[s])
        inner = compact(passes(halves, halves, dot_nt))
        spread = compact(jnp.broadcast_to(column(1, s), (rows, rows))) - running[s : s + 1]
        below = jnp.where(strict, jnp.exp(jnp.where(strict, spread, 0.0)), 0.0)
        n_mat = compact(jnp.broadcast_to(column(0, s), (rows, rows))) * inner * below
        n_mats.append(n_mat)
    near = row_c // 8 == inside // 8
    small = [split(jnp.where(near, n_mat, 0.0)) for n_mat in n_mats]
    squares = [passes(m, diagonal(m)) for m in small]
    for s in range(seqs):
        square = split(squares[s])
        spread2 = diagonal(square)
        fourth = passes(square, spread2)
        start = eye - jnp.where(near, n_mats[s], 0.0) + squares[s] - passes(small[s], spread2)
        solves.append(start + passes(split(start), diagonal(split(fourth))))
    depth = 3
    while 1 << depth < BLOCK:
        ri = lax.shift_right_logical(row_c, depth)
        ci = lax.shift_right_logical(inside, depth)
        mask = jnp.logical_and(ri == ci + 1, lax.bitwise_and(ci, 1) == 0)
        for s in range(seqs):
            t_mat = split(solves[s])
            inner = passes(split(jnp.where(mask, n_mats[s], 0.0)), diagonal(t_mat))
            solves[s] = solves[s] - passes(t_mat, diagonal(split(inner)))
        depth += 1

    head_eye = jnp.where(iota((head, head), 0) == iota((head, head), 1), 1.0, 0.0)
    row_b = iota((rows, 1), 0) // BLOCK
    inverse = [diagonal(split(t_mat)) for t_mat in solves]
    pieces = []
    for s in range(seqs):
        keys = k_ref[s]
        right = jnp.concatenate([keys * column(2, s), v_ref[s] * column(0, s)], axis=1)
        solved = passes(inverse[s], split(right))
        kept = keys * column(3, s)
        spans = jnp.concatenate(
            [jnp.where(row_b == b, kept, 0.0) for b in range(blocks)], axis=1
        )
        moved = passes(split(jnp.transpose(solved)), split(spans))
        piece = []
        for b in range(blocks):
            decay = jnp.exp(total[s : s + 1, b * BLOCK : b * BLOCK + 1])
            part = moved[:, b * head : (b + 1) * head]
            piece.append((decay * head_eye - part[:head], part[head:]))
        pieces.append(piece)
    while len(pieces[0]) > 1:
        for s in range(seqs):
            merged = []
            for early, late in zip(pieces[s][0::2], pieces[s][1::2]):
                both = product(jnp.concatenate(early, axis=0), late[0])
                merged.append((both[:head], both[head:] + late[1]))
            pieces[s] = merged
    for s in range(seqs):
        ab_ref[s, 0], ab_ref[s, 1] = pieces[s][0]

    def chain(s, half):
        return pltpu.make_async_remote_copy(
            src_ref=tx_ref.at[s, half],
            dst_ref=rx_ref.at[s, half],
            send_sem=send_x.at[s, half],
            recv_sem=recv_x.at[s, half],
            device_id=at(lax.rem(me + 1, count)),
            device_id_type=MESH,
        )

    def push(s):
        return pltpu.make_async_remote_copy(
            src_ref=ab_ref.at[s, 1],
            dst_ref=first_ref.at[s],
            send_sem=send_f.at[s],
            recv_sem=recv_f.at[s],
            device_id=at(last_one),
            device_id_type=MESH,
        )

    decoded = pltpu.make_async_remote_copy(
        src_ref=new_tx,
        dst_ref=new_rx,
        send_sem=send_n,
        recv_sem=recv_n,
        device_id=at(last_one),
        device_id_type=MESH,
    )

    def rows_to(s, k):
        to = lax.rem(me + k, count)
        return pltpu.make_async_remote_copy(
            src_ref=out_tx.at[s, to],
            dst_ref=out_rx.at[s],
            send_sem=send_o.at[s, k],
            recv_sem=recv_o.at[s],
            device_id=at(to),
            device_id_type=MESH,
        )

    @pl.when(is_first)
    def _():
        pl.semaphore_wait(barrier, 1)
        for s in range(seqs):
            push(s).start()

    @pl.when(in_chain)
    def _():
        pl.semaphore_wait(barrier, 1)
        for half in range(2):
            for s in range(seqs):

                @pl.when(is_second)
                def _():
                    tx_ref[s, half] = ab_ref[s, half]

                @pl.when(jnp.logical_not(is_second))
                def _():
                    chain(s, half).wait_recv()
                    moved = product(rx_ref[s, half], ab_ref[s, 0])
                    tx_ref[s, half] = moved + ab_ref[s, 1] if half else moved

                chain(s, half).start()

    @pl.when(is_decoder)
    def _():
        for copy in load_dec:
            copy.wait()
        dec = dec_ref[...]
        new_kv = silu(dot(dec, wkv_ref[...]))
        new_key = unit_rows(new_kv[:, :head])
        new_value = new_kv[:, head:]
        query = silu(dot(dec, wq_ref[...]))
        both = dot_nt(gate_ref[...], dec)
        row_n = iota((gates, seqs), 0)
        picked = [
            jnp.sum(jnp.where(row_n == local_head, part, 0.0), axis=0, keepdims=True)
            for part in (both[:gates], both[gates:])
        ]
        new_beta = jax.nn.sigmoid(picked[0] - write_offset)
        keep = jnp.exp(-rate * softplus(picked[1]))
        for s in range(seqs):
            one = slice(s, s + 1)
            new_tx[s, 0:1] = new_key[one]
            new_tx[s, 1:2] = query[one]
            new_tx[s, 2:3] = new_value[one]
            new_tx[s, 3:4] = jnp.broadcast_to(new_beta[:, one], (1, head))
            new_tx[s, 4:5] = jnp.broadcast_to(keep[:, one], (1, head))
            new_tx[s, 5:8] = jnp.zeros((3, head), F32)
        decoded.start()

    @pl.when(is_last)
    def _():
        pl.semaphore_wait(barrier, count - 1)
        load_r.wait()
        decoded.wait_recv()
        ahead = []
        for s in range(seqs):
            step, own = split(ab_ref[s, 0]), ab_ref[s, 1]
            new = split(new_rx[s])
            read_step = passes(new, step, dot_nt)
            ahead.append((step, split(read_step), passes(new, split(own), dot_nt)))
        joins = []
        for s in range(seqs):
            chain(s, 0).wait_recv()
            push(s).wait_recv()
            joins.append(product(first_ref[s], rx_ref[s, 0]))
        for s in range(seqs):
            step, read_step, read_own = ahead[s]
            chain(s, 1).wait_recv()
            joined = split(joins[s] + rx_ref[s, 1])
            flipped = passes(joined, step) + ab_ref[s, 1]
            reads = passes(read_step, joined, dot_nt) + read_own
            new = new_rx[s]
            final = jnp.transpose(flipped)
            key_read, query_read = reads[0:1], reads[1:2]
            value, beta, hold = new[2:3], new[3:4], new[4:5]
            inter = jnp.sum(new[0:1] * new[1:2], axis=-1, keepdims=True)
            key_col = jnp.transpose(new)[:, 0:1]
            cache = hold * final + key_col * (beta * value - (hold * beta) * key_read)
            mixed = hold * query_read - (hold * beta * inter) * key_read + (beta * inter) * value
            scale = lax.rsqrt(jnp.sum(mixed * mixed, axis=-1, keepdims=True) / head + epsilon)
            read = mixed * scale * gain_ref[...]
            each = head // count
            out_tx[s, :, :each] = cache.reshape(count, each, head)
            out_tx[s, :, each:] = jnp.broadcast_to(read.reshape(1, 1, head), (count, each, head))
            for k in range(1, count):
                rows_to(s, k).start()
            out_rx[s] = out_tx[s, last_one]

    for s in range(seqs):

        @pl.when(jnp.logical_not(is_last))
        def _():
            rows_to(s, 1).wait_recv()

        each = head // count
        cache_ref[s, 0] = out_rx[s, :each].astype(BF16)
        read_ref[s : s + 1] = out_rx[s, each : each + 1].astype(BF16)

    @pl.when(jnp.logical_not(is_last))
    def _():
        load_r.wait()

    @pl.when(is_first)
    def _():
        for s in range(seqs):
            push(s).wait_send()

    @pl.when(is_decoder)
    def _():
        decoded.wait_send()

    @pl.when(in_chain)
    def _():
        for half in range(2):
            for s in range(seqs):
                chain(s, half).wait_send()

    @pl.when(is_last)
    def _():
        for s in range(seqs):
            for k in range(1, count):
                rows_to(s, k).wait_send()


def per_device(
    tokens,
    decoded_input,
    query_weight,
    key_weight,
    value_weight,
    gate_weight,
    head_decay_rate,
    extra_log_decay,
    read_norm_gain,
):
    seqs, rows, width = tokens.shape
    head = key_weight.shape[1]
    count = lax.axis_size("sp")
    each = head // count
    gates = gate_weight.transpose(1, 2, 0).reshape(-1, width)
    vmem = pl.BlockSpec(memory_space=pltpu.VMEM)
    hbm = pl.BlockSpec(memory_space=pltpu.HBM)
    dma = pltpu.SemaphoreType.DMA
    return pl.pallas_call(
        functools.partial(kernel, seqs, rows, count),
        out_shape=(
            jax.ShapeDtypeStruct((seqs, 1, each, head), BF16),
            jax.ShapeDtypeStruct((seqs, head), BF16),
        ),
        in_specs=[hbm] * 9,
        out_specs=(vmem, vmem),
        scratch_shapes=[
            pltpu.VMEM((seqs, rows, width), BF16),
            pltpu.VMEM((seqs, width), BF16),
            pltpu.VMEM((width, 2 * head), BF16),
            pltpu.VMEM((width, head), BF16),
            pltpu.VMEM((2 * GROUP, width), BF16),
            pltpu.SMEM((1,), F32),
            pltpu.VMEM((seqs, 1, rows), F32),
            pltpu.VMEM((1, head), F32),
            pltpu.VMEM((seqs, rows, head), F32),
            pltpu.VMEM((seqs, rows, head), F32),
            pltpu.VMEM((seqs, 2, head, head), F32),
            pltpu.VMEM((seqs, 2, head, head), F32),
            pltpu.VMEM((seqs, 2, head, head), F32),
            pltpu.VMEM((seqs, head, head), F32),
            pltpu.VMEM((seqs, 8, head), F32),
            pltpu.VMEM((seqs, 8, head), F32),
            pltpu.VMEM((seqs, count, 2 * each, head), F32),
            pltpu.VMEM((seqs, 2 * each, head), F32),
            dma((8 + CHUNKS * (seqs + 4),)),
            dma((seqs, 2)),
            dma((seqs, 2)),
            dma((seqs,)),
            dma((seqs,)),
            dma,
            dma,
            dma((seqs, count)),
            dma((seqs,)),
        ],
        compiler_params=pltpu.CompilerParams(
            collective_id=0, has_side_effects=True, vmem_limit_bytes=GRANT
        ),
    )(*[x if x.shape == (1,) else pltpu.with_memory_space_constraint(x, pltpu.HBM) for x in (
        tokens,
        decoded_input,
        query_weight,
        key_weight,
        value_weight,
        gates,
        head_decay_rate,
        extra_log_decay,
        read_norm_gain.reshape(1, head),
    )]    )


def solution(mesh):
    in_specs = (
        P("grp", "sp", None),
        P("grp", None),
        P(None, "tp"),
        P(None, "tp"),
        P(None, "tp"),
        P(),
        P("tp"),
        P("grp", "tp", "sp"),
        P(),
    )
    out_specs = (P("grp", "tp", "sp", None), P("grp", "tp"))
    return jax.shard_map(
        per_device, mesh=mesh, in_specs=in_specs, out_specs=out_specs, check_vma=False
    )
```

```python
import functools

import jax
import jax.numpy as jnp
from jax import lax
from jax.experimental import pallas as pl
from jax.experimental.pallas import tpu as pltpu
from jax.sharding import PartitionSpec as P

MESH = pl.DeviceIdType.MESH
F32 = jnp.float32
BF16 = jnp.bfloat16
epsilon = 1e-06
write_offset = 5.0
BLOCK = 64
CHUNKS = 4
GROUP = 8
GRANT = 24 << 20


def split(x):
    hi = x.astype(BF16)
    lo = (x - hi.astype(F32)).astype(BF16)
    return hi, lo


def dot(a, b):
    return jnp.dot(a, b, preferred_element_type=F32)


def dot_nt(a, b):
    return lax.dot_general(a, b, (((1,), (1,)), ((), ())), preferred_element_type=F32)


def passes(a, b, one=dot):
    rows = a[0].shape[0]
    both = one(jnp.concatenate([a[0], a[1]], axis=0), b[0])
    return both[:rows] + (one(a[0], b[1]) + both[rows:])


def product(a, b, one=dot):
    return passes(split(a), split(b), one)


def silu(x):
    return x * jax.nn.sigmoid(x)


def softplus(x):
    return jnp.maximum(x, 0.0) + jnp.log1p(jnp.exp(-jnp.abs(x)))


def unit_rows(x):
    return x * lax.rsqrt(jnp.sum(x * x, axis=-1, keepdims=True) + epsilon)


def iota(shape, dim):
    return lax.broadcasted_iota(jnp.int32, shape, dim)


def kernel(
    seqs,
    rows,
    count,
    tok_hbm,
    dec_hbm,
    wq_hbm,
    wk_hbm,
    wv_hbm,
    gate_hbm,
    rate_hbm,
    extra_hbm,
    gain_hbm,
    cache_ref,
    read_ref,
    x_ref,
    dec_ref,
    wkv_ref,
    wq_ref,
    gate_ref,
    rate_ref,
    extra_ref,
    gain_ref,
    k_ref,
    v_ref,
    ab_ref,
    rx_ref,
    tx_ref,
    first_ref,
    new_tx,
    new_rx,
    out_tx,
    out_rx,
    load_sem,
    send_x,
    recv_x,
    send_f,
    recv_f,
    send_n,
    recv_n,
    send_o,
    recv_o,
):
    me = lax.axis_index("sp")
    head_index = lax.axis_index("tp")
    head = k_ref.shape[-1]
    gates = GROUP
    heads = gate_hbm.shape[0] // 2
    first = pl.multiple_of(head_index // GROUP * GROUP, GROUP)
    local_head = lax.rem(head_index, GROUP)
    last_one = count - 1
    is_first = me == 0
    is_second = me == 1
    is_decoder = me == 0
    is_last = me == last_one
    in_chain = jnp.logical_and(me > 0, me < last_one)

    def load(source, target, place):
        copy = pltpu.make_async_copy(source, target, load_sem.at[place])
        copy.start()
        return copy

    width = x_ref.shape[-1]
    wide = width // CHUNKS
    loads = []
    for c in range(CHUNKS):
        cut = pl.ds(c * wide, wide)
        pairs = [
            (wk_hbm.at[cut], wkv_ref.at[cut, pl.ds(0, head)]),
            (wv_hbm.at[cut], wkv_ref.at[cut, pl.ds(head, head)]),
        ]
        pairs += [(tok_hbm.at[s, :, cut], x_ref.at[s, :, cut]) for s in range(seqs)]
        pairs += [
            (gate_hbm.at[pl.ds(first + g // GROUP * heads, GROUP), cut], gate_ref.at[pl.ds(g, GROUP), cut])
            for g in (0, GROUP)
        ]
        loads.append(
            [load(pair[0], pair[1], 8 + c * len(pairs) + i) for i, pair in enumerate(pairs)]
        )
    load_g = [load(rate_hbm, rate_ref, 4), load(extra_hbm, extra_ref, 5)]
    load_r = load(gain_hbm, gain_ref, 6)
    load_dec = [
        pltpu.make_async_copy(dec_hbm, dec_ref, load_sem.at[7]),
        pltpu.make_async_copy(wq_hbm, wq_ref, load_sem.at[3]),
    ]

    @pl.when(is_decoder)
    def _():
        for copy in load_dec:
            copy.start()


    def at(index):
        return {"sp": index}

    barrier = pltpu.get_barrier_semaphore()

    def greet(index):
        pl.semaphore_signal(barrier, inc=1, device_id=at(index), device_id_type=MESH)

    @pl.when(me >= 2)
    def _():
        greet(me - 1)

    @pl.when(is_last)
    def _():
        greet(0)

    @pl.when(jnp.logical_not(is_last))
    def _():
        greet(last_one)

    row_g = iota((gates, rows), 0)
    sums = [None] * seqs
    gate_sums = [None] * seqs
    for c in range(CHUNKS):
        for copy in loads[c]:
            copy.wait()
        cut = slice(c * wide, (c + 1) * wide)
        for s in range(seqs):
            part = dot(x_ref[s, :, cut], wkv_ref[cut])
            sums[s] = part if c == 0 else sums[s] + part
            part = dot_nt(gate_ref[:, cut], x_ref[s, :, cut])
            gate_sums[s] = part if c == 0 else gate_sums[s] + part
    for copy in load_g:
        copy.wait()
    gate_rows = []
    for s in range(seqs):
        kv = silu(sums[s])
        k_ref[s] = unit_rows(kv[:, :head])
        v_ref[s] = kv[:, head:]
        picked = [
            jnp.sum(jnp.where(row_g == local_head, part, 0.0), axis=0, keepdims=True)
            for part in (gate_sums[s][:gates], gate_sums[s][gates:])
        ]
        gate_rows.append(picked)
    rate = rate_ref[0]
    betas = [jax.nn.sigmoid(g[0] - write_offset) for g in gate_rows]
    decays = [-rate * softplus(g[1]) + extra_ref[s] for s, g in enumerate(gate_rows)]
    stacked = jnp.concatenate(decays, axis=0)
    hi, rest = split(stacked)
    rest32 = stacked - hi.astype(F32)
    lo = (rest32 - rest.astype(F32)).astype(BF16)
    parts = (hi, rest, lo)
    row_i = iota((rows, rows), 0)
    col_i = iota((rows, rows), 1)
    together = row_i // BLOCK == col_i // BLOCK
    upto = jnp.where(jnp.logical_and(together, row_i <= col_i), 1.0, 0.0).astype(BF16)
    whole = jnp.where(together, 1.0, 0.0).astype(BF16)
    running = sum(dot(part, upto) for part in parts)
    total = sum(dot(part, whole) for part in parts)
    grown = jnp.exp(running)
    packed = jnp.concatenate(
        betas
        + [running]
        + [betas[s] * grown[s : s + 1] for s in range(seqs)]
        + [jnp.exp(total - running)],
        axis=0,
    )
    columns = jnp.transpose(packed)

    def column(kind, s):
        place = kind * seqs + s
        return columns[:, place : place + 1]

    blocks = rows // BLOCK
    row_c = iota((BLOCK, rows), 0)
    lane_c = iota((BLOCK, rows), 1)
    inside = lax.bitwise_and(lane_c, BLOCK - 1)
    owner = lane_c // BLOCK
    own_lanes = [jnp.where(owner == b, 1.0, 0.0).astype(BF16) for b in range(blocks)]
    strict = row_c > inside
    eye = jnp.where(row_c == inside, 1.0, 0.0)

    def compact(full):
        out = jnp.where(owner == 0, full[:BLOCK], 0.0)
        for b in range(1, blocks):
            out = jnp.where(owner == b, full[b * BLOCK : (b + 1) * BLOCK], out)
        return out

    def diagonal(pair):
        return [jnp.concatenate([part * own for own in own_lanes], axis=0) for part in pair]

    head_eye = jnp.where(iota((head, head), 0) == iota((head, head), 1), 1.0, 0.0)
    row_b = iota((rows, 1), 0) // BLOCK
    near = row_c // 8 == inside // 8

    def solve(s):
        keys = k_ref[s]
        halves = split(keys)
        inner = compact(passes(halves, halves, dot_nt))
        yield
        spread = compact(jnp.broadcast_to(column(1, s), (rows, rows))) - running[s : s + 1]
        below = jnp.where(strict, jnp.exp(jnp.where(strict, spread, 0.0)), 0.0)
        yield
        n_mat = compact(jnp.broadcast_to(column(0, s), (rows, rows))) * inner * below
        small = jnp.where(near, n_mat, 0.0)
        parts = split(small)
        square = passes(parts, diagonal(parts))
        yield
        halves = split(square)
        spread2 = diagonal(halves)
        fourth = passes(halves, spread2)
        yield
        start = eye - small + square - passes(parts, spread2)
        yield
        solved = start + passes(split(start), diagonal(split(fourth)))
        yield
        own = split(solved)
        spread_own = diagonal(own)
        lower = jnp.where(near, 0.0, n_mat)
        first_power = passes(own, diagonal(split(lower)))
        yield
        parts = split(first_power)
        square = passes(parts, diagonal(parts))
        yield
        halves = split(square)
        spread2 = diagonal(halves)
        fourth = passes(halves, spread2)
        start = eye - first_power + square - passes(parts, spread2)
        yield
        chain8 = start + passes(split(start), diagonal(split(fourth)))
        yield
        solved = passes(split(chain8), spread_own)
        yield
        right = jnp.concatenate([keys * column(2, s), v_ref[s] * column(0, s)], axis=1)
        deltas = passes(diagonal(split(solved)), split(right))
        yield
        kept = keys * column(3, s)
        spans = jnp.concatenate(
            [jnp.where(row_b == b, kept, 0.0) for b in range(blocks)], axis=1
        )
        moved = passes(split(jnp.transpose(deltas)), split(spans))
        yield
        pieces = []
        for b in range(blocks):
            decay = jnp.exp(total[s : s + 1, b * BLOCK : b * BLOCK + 1])
            part = moved[:, b * head : (b + 1) * head]
            pieces.append((decay * head_eye - part[:head], part[head:]))
        while len(pieces) > 1:
            merged = []
            for early, late in zip(pieces[0::2], pieces[1::2]):
                both = product(jnp.concatenate(early, axis=0), late[0])
                merged.append((both[:head], both[head:] + late[1]))
            pieces = merged
            yield
        ab_ref[s, 0], ab_ref[s, 1] = pieces[0]
        yield

    for _ in zip(*[solve(s) for s in range(seqs)]):
        pass

    def chain(s, half):
        return pltpu.make_async_remote_copy(
            src_ref=tx_ref.at[s, half],
            dst_ref=rx_ref.at[s, half],
            send_sem=send_x.at[s, half],
            recv_sem=recv_x.at[s, half],
            device_id=at(lax.rem(me + 1, count)),
            device_id_type=MESH,
        )

    def push(s):
        return pltpu.make_async_remote_copy(
            src_ref=ab_ref.at[s, 1],
            dst_ref=first_ref.at[s],
            send_sem=send_f.at[s],
            recv_sem=recv_f.at[s],
            device_id=at(last_one),
            device_id_type=MESH,
        )

    decoded = pltpu.make_async_remote_copy(
        src_ref=new_tx,
        dst_ref=new_rx,
        send_sem=send_n,
        recv_sem=recv_n,
        device_id=at(last_one),
        device_id_type=MESH,
    )

    def rows_to(s, k):
        to = lax.rem(me + k, count)
        return pltpu.make_async_remote_copy(
            src_ref=out_tx.at[s, to],
            dst_ref=out_rx.at[s],
            send_sem=send_o.at[s, k],
            recv_sem=recv_o.at[s],
            device_id=at(to),
            device_id_type=MESH,
        )

    @pl.when(is_first)
    def _():
        pl.semaphore_wait(barrier, 1)
        for s in range(seqs):
            push(s).start()

    @pl.when(in_chain)
    def _():
        pl.semaphore_wait(barrier, 1)
        for half in range(2):
            for s in range(seqs):

                @pl.when(is_second)
                def _():
                    tx_ref[s, half] = ab_ref[s, half]

                @pl.when(jnp.logical_not(is_second))
                def _():
                    chain(s, half).wait_recv()
                    moved = product(rx_ref[s, half], ab_ref[s, 0])
                    tx_ref[s, half] = moved + ab_ref[s, 1] if half else moved

                chain(s, half).start()

    @pl.when(is_decoder)
    def _():
        for copy in load_dec:
            copy.wait()
        dec = dec_ref[...]
        new_kv = silu(dot(dec, wkv_ref[...]))
        new_key = unit_rows(new_kv[:, :head])
        new_value = new_kv[:, head:]
        query = silu(dot(dec, wq_ref[...]))
        both = dot_nt(gate_ref[...], dec)
        row_n = iota((gates, seqs), 0)
        picked = [
            jnp.sum(jnp.where(row_n == local_head, part, 0.0), axis=0, keepdims=True)
            for part in (both[:gates], both[gates:])
        ]
        new_beta = jax.nn.sigmoid(picked[0] - write_offset)
        keep = jnp.exp(-rate * softplus(picked[1]))
        for s in range(seqs):
            one = slice(s, s + 1)
            new_tx[s, 0:1] = new_key[one]
            new_tx[s, 1:2] = query[one]
            new_tx[s, 2:3] = new_value[one]
            new_tx[s, 3:4] = jnp.broadcast_to(new_beta[:, one], (1, head))
            new_tx[s, 4:5] = jnp.broadcast_to(keep[:, one], (1, head))
            new_tx[s, 5:8] = jnp.zeros((3, head), F32)
        decoded.start()

    @pl.when(is_last)
    def _():
        pl.semaphore_wait(barrier, count - 1)
        load_r.wait()
        decoded.wait_recv()
        ahead = []
        for s in range(seqs):
            step, own = split(ab_ref[s, 0]), ab_ref[s, 1]
            new = split(new_rx[s])
            read_step = passes(new, step, dot_nt)
            ahead.append((step, split(read_step), passes(new, split(own), dot_nt)))
        joins = []
        for s in range(seqs):
            chain(s, 0).wait_recv()
            push(s).wait_recv()
            joins.append(product(first_ref[s], rx_ref[s, 0]))
        for s in range(seqs):
            step, read_step, read_own = ahead[s]
            chain(s, 1).wait_recv()
            joined = split(joins[s] + rx_ref[s, 1])
            flipped = passes(joined, step) + ab_ref[s, 1]
            reads = passes(read_step, joined, dot_nt) + read_own
            new = new_rx[s]
            final = jnp.transpose(flipped)
            key_read, query_read = reads[0:1], reads[1:2]
            value, beta, hold = new[2:3], new[3:4], new[4:5]
            inter = jnp.sum(new[0:1] * new[1:2], axis=-1, keepdims=True)
            key_col = jnp.transpose(new)[:, 0:1]
            cache = hold * final + key_col * (beta * value - (hold * beta) * key_read)
            mixed = hold * query_read - (hold * beta * inter) * key_read + (beta * inter) * value
            scale = lax.rsqrt(jnp.sum(mixed * mixed, axis=-1, keepdims=True) / head + epsilon)
            read = mixed * scale * gain_ref[...]
            each = head // count
            out_tx[s, :, :each] = cache.reshape(count, each, head)
            out_tx[s, :, each:] = jnp.broadcast_to(read.reshape(1, 1, head), (count, each, head))
            for k in range(1, count):
                rows_to(s, k).start()
            out_rx[s] = out_tx[s, last_one]

    for s in range(seqs):

        @pl.when(jnp.logical_not(is_last))
        def _():
            rows_to(s, 1).wait_recv()

        each = head // count
        cache_ref[s, 0] = out_rx[s, :each].astype(BF16)
        read_ref[s : s + 1] = out_rx[s, each : each + 1].astype(BF16)

    @pl.when(jnp.logical_not(is_last))
    def _():
        load_r.wait()

    @pl.when(is_first)
    def _():
        for s in range(seqs):
            push(s).wait_send()

    @pl.when(is_decoder)
    def _():
        decoded.wait_send()

    @pl.when(in_chain)
    def _():
        for half in range(2):
            for s in range(seqs):
                chain(s, half).wait_send()

    @pl.when(is_last)
    def _():
        for s in range(seqs):
            for k in range(1, count):
                rows_to(s, k).wait_send()


def per_device(
    tokens,
    decoded_input,
    query_weight,
    key_weight,
    value_weight,
    gate_weight,
    head_decay_rate,
    extra_log_decay,
    read_norm_gain,
):
    seqs, rows, width = tokens.shape
    head = key_weight.shape[1]
    count = lax.axis_size("sp")
    each = head // count
    gates = gate_weight.transpose(1, 2, 0).reshape(-1, width)
    vmem = pl.BlockSpec(memory_space=pltpu.VMEM)
    hbm = pl.BlockSpec(memory_space=pltpu.HBM)
    dma = pltpu.SemaphoreType.DMA
    return pl.pallas_call(
        functools.partial(kernel, seqs, rows, count),
        out_shape=(
            jax.ShapeDtypeStruct((seqs, 1, each, head), BF16),
            jax.ShapeDtypeStruct((seqs, head), BF16),
        ),
        in_specs=[hbm] * 9,
        out_specs=(vmem, vmem),
        scratch_shapes=[
            pltpu.VMEM((seqs, rows, width), BF16),
            pltpu.VMEM((seqs, width), BF16),
            pltpu.VMEM((width, 2 * head), BF16),
            pltpu.VMEM((width, head), BF16),
            pltpu.VMEM((2 * GROUP, width), BF16),
            pltpu.SMEM((1,), F32),
            pltpu.VMEM((seqs, 1, rows), F32),
            pltpu.VMEM((1, head), F32),
            pltpu.VMEM((seqs, rows, head), F32),
            pltpu.VMEM((seqs, rows, head), F32),
            pltpu.VMEM((seqs, 2, head, head), F32),
            pltpu.VMEM((seqs, 2, head, head), F32),
            pltpu.VMEM((seqs, 2, head, head), F32),
            pltpu.VMEM((seqs, head, head), F32),
            pltpu.VMEM((seqs, 8, head), F32),
            pltpu.VMEM((seqs, 8, head), F32),
            pltpu.VMEM((seqs, count, 2 * each, head), F32),
            pltpu.VMEM((seqs, 2 * each, head), F32),
            dma((8 + CHUNKS * (seqs + 4),)),
            dma((seqs, 2)),
            dma((seqs, 2)),
            dma((seqs,)),
            dma((seqs,)),
            dma,
            dma,
            dma((seqs, count)),
            dma((seqs,)),
        ],
        compiler_params=pltpu.CompilerParams(
            collective_id=0, has_side_effects=True, vmem_limit_bytes=GRANT
        ),
    )(*[x if x.shape == (1,) else pltpu.with_memory_space_constraint(x, pltpu.HBM) for x in (
        tokens,
        decoded_input,
        query_weight,
        key_weight,
        value_weight,
        gates,
        head_decay_rate,
        extra_log_decay,
        read_norm_gain.reshape(1, head),
    )]    )


def solution(mesh):
    in_specs = (
        P("grp", "sp", None),
        P("grp", None),
        P(None, "tp"),
        P(None, "tp"),
        P(None, "tp"),
        P(),
        P("tp"),
        P("grp", "tp", "sp"),
        P(),
    )
    out_specs = (P("grp", "tp", "sp", None), P("grp", "tp"))
    return jax.shard_map(
        per_device, mesh=mesh, in_specs=in_specs, out_specs=out_specs, check_vma=False
    )
```

```python
import functools

import jax
import jax.numpy as jnp
from jax import lax
from jax.experimental import pallas as pl
from jax.experimental.pallas import tpu as pltpu
from jax.sharding import PartitionSpec as P

MESH = pl.DeviceIdType.MESH
F32 = jnp.float32
BF16 = jnp.bfloat16
epsilon = 1e-06
write_offset = 5.0
BLOCK = 64
CHUNKS = 4
GROUP = 8
GRANT = 24 << 20


def split(x):
    hi = x.astype(BF16)
    lo = (x - hi.astype(F32)).astype(BF16)
    return hi, lo


def dot(a, b):
    return jnp.dot(a, b, preferred_element_type=F32)


def dot_nt(a, b):
    return lax.dot_general(a, b, (((1,), (1,)), ((), ())), preferred_element_type=F32)


def passes(a, b, one=dot):
    if a[0].shape[1] == 128:
        wide = jnp.concatenate(a, axis=1)
        twice = jnp.concatenate([b[0], b[0]], axis=0 if one is dot else 1)
        return one(wide, twice) + one(a[0], b[1])
    rows = a[0].shape[0]
    both = one(jnp.concatenate([a[0], a[1]], axis=0), b[0])
    return both[:rows] + (one(a[0], b[1]) + both[rows:])


def product(a, b, one=dot):
    return passes(split(a), split(b), one)


def silu(x):
    return x * jax.nn.sigmoid(x)


def softplus(x):
    return jnp.maximum(x, 0.0) + jnp.log1p(jnp.exp(-jnp.abs(x)))


def unit_rows(x):
    return x * lax.rsqrt(jnp.sum(x * x, axis=-1, keepdims=True) + epsilon)


def iota(shape, dim):
    return lax.broadcasted_iota(jnp.int32, shape, dim)


def kernel(
    seqs,
    rows,
    count,
    tok_hbm,
    dec_hbm,
    wq_hbm,
    wk_hbm,
    wv_hbm,
    gate_hbm,
    rate_hbm,
    extra_hbm,
    gain_hbm,
    cache_ref,
    read_ref,
    x_ref,
    dec_ref,
    wkv_ref,
    wq_ref,
    gate_ref,
    rate_ref,
    extra_ref,
    gain_ref,
    k_ref,
    v_ref,
    ab_ref,
    rx_ref,
    tx_ref,
    first_ref,
    new_tx,
    new_rx,
    out_tx,
    out_rx,
    load_sem,
    send_x,
    recv_x,
    send_f,
    recv_f,
    send_n,
    recv_n,
    send_o,
    recv_o,
):
    me = lax.axis_index("sp")
    head_index = lax.axis_index("tp")
    head = k_ref.shape[-1]
    gates = GROUP
    heads = gate_hbm.shape[0] // 2
    first = pl.multiple_of(head_index // GROUP * GROUP, GROUP)
    local_head = lax.rem(head_index, GROUP)
    last_one = count - 1
    is_first = me == 0
    is_second = me == 1
    is_decoder = me == 0
    is_last = me == last_one
    in_chain = jnp.logical_and(me > 0, me < last_one)

    def load(source, target, place):
        copy = pltpu.make_async_copy(source, target, load_sem.at[place])
        copy.start()
        return copy

    width = x_ref.shape[-1]
    wide = width // CHUNKS
    loads = []
    for c in range(CHUNKS):
        cut = pl.ds(c * wide, wide)
        pairs = [
            (wk_hbm.at[cut], wkv_ref.at[cut, pl.ds(0, head)]),
            (wv_hbm.at[cut], wkv_ref.at[cut, pl.ds(head, head)]),
        ]
        pairs += [(tok_hbm.at[s, :, cut], x_ref.at[s, :, cut]) for s in range(seqs)]
        pairs += [
            (gate_hbm.at[pl.ds(first + g // GROUP * heads, GROUP), cut], gate_ref.at[pl.ds(g, GROUP), cut])
            for g in (0, GROUP)
        ]
        loads.append(
            [load(pair[0], pair[1], 8 + c * len(pairs) + i) for i, pair in enumerate(pairs)]
        )
    load_g = [load(rate_hbm, rate_ref, 4), load(extra_hbm, extra_ref, 5)]
    load_r = load(gain_hbm, gain_ref, 6)
    load_dec = [
        pltpu.make_async_copy(dec_hbm, dec_ref, load_sem.at[7]),
        pltpu.make_async_copy(wq_hbm, wq_ref, load_sem.at[3]),
    ]

    @pl.when(is_decoder)
    def _():
        for copy in load_dec:
            copy.start()


    def at(index):
        return {"sp": index}

    barrier = pltpu.get_barrier_semaphore()

    def greet(index):
        pl.semaphore_signal(barrier, inc=1, device_id=at(index), device_id_type=MESH)

    @pl.when(me >= 2)
    def _():
        greet(me - 1)

    @pl.when(is_last)
    def _():
        greet(0)

    @pl.when(jnp.logical_not(is_last))
    def _():
        greet(last_one)

    row_g = iota((gates, rows), 0)
    sums = [None] * seqs
    gate_sums = [None] * seqs
    for c in range(CHUNKS):
        for copy in loads[c]:
            copy.wait()
        cut = slice(c * wide, (c + 1) * wide)
        for s in range(seqs):
            part = dot(x_ref[s, :, cut], wkv_ref[cut])
            sums[s] = part if c == 0 else sums[s] + part
            part = dot_nt(gate_ref[:, cut], x_ref[s, :, cut])
            gate_sums[s] = part if c == 0 else gate_sums[s] + part
    for copy in load_g:
        copy.wait()
    gate_rows = []
    for s in range(seqs):
        kv = silu(sums[s])
        k_ref[s] = unit_rows(kv[:, :head])
        v_ref[s] = kv[:, head:]
        picked = [
            jnp.sum(jnp.where(row_g == local_head, part, 0.0), axis=0, keepdims=True)
            for part in (gate_sums[s][:gates], gate_sums[s][gates:])
        ]
        gate_rows.append(picked)
    rate = rate_ref[0]
    betas = [jax.nn.sigmoid(g[0] - write_offset) for g in gate_rows]
    decays = [-rate * softplus(g[1]) + extra_ref[s] for s, g in enumerate(gate_rows)]
    stacked = jnp.concatenate(decays, axis=0)
    hi, rest = split(stacked)
    rest32 = stacked - hi.astype(F32)
    lo = (rest32 - rest.astype(F32)).astype(BF16)
    parts = (hi, rest, lo)
    row_i = iota((rows, rows), 0)
    col_i = iota((rows, rows), 1)
    together = row_i // BLOCK == col_i // BLOCK
    upto = jnp.where(jnp.logical_and(together, row_i <= col_i), 1.0, 0.0).astype(BF16)
    whole = jnp.where(together, 1.0, 0.0).astype(BF16)
    running = sum(dot(part, upto) for part in parts)
    total = sum(dot(part, whole) for part in parts)
    grown = jnp.exp(running)
    packed = jnp.concatenate(
        betas
        + [running]
        + [betas[s] * grown[s : s + 1] for s in range(seqs)]
        + [jnp.exp(total - running)],
        axis=0,
    )
    columns = jnp.transpose(packed)

    def column(kind, s):
        place = kind * seqs + s
        return columns[:, place : place + 1]

    blocks = rows // BLOCK
    row_c = iota((BLOCK, rows), 0)
    lane_c = iota((BLOCK, rows), 1)
    inside = lax.bitwise_and(lane_c, BLOCK - 1)
    owner = lane_c // BLOCK
    own_lanes = [owner == b for b in range(blocks)]
    strict = row_c > inside
    eye = jnp.where(row_c == inside, 1.0, 0.0)

    def compact(full):
        out = jnp.where(owner == 0, full[:BLOCK], 0.0)
        for b in range(1, blocks):
            out = jnp.where(owner == b, full[b * BLOCK : (b + 1) * BLOCK], out)
        return out

    def diagonal(pair):
        return [jnp.concatenate([jnp.where(own, part, jnp.zeros_like(part)) for own in own_lanes], axis=0) for part in pair]

    head_eye = jnp.where(iota((head, head), 0) == iota((head, head), 1), 1.0, 0.0)
    row_b = iota((rows, 1), 0) // BLOCK
    near = row_c // 8 == inside // 8

    def solve(s):
        keys = k_ref[s]
        halves = split(keys)
        inner = compact(passes(halves, halves, dot_nt))
        yield
        spread = compact(jnp.broadcast_to(column(1, s), (rows, rows))) - running[s : s + 1]
        below = jnp.where(strict, jnp.exp(jnp.where(strict, spread, 0.0)), 0.0)
        yield
        n_mat = compact(jnp.broadcast_to(column(0, s), (rows, rows))) * inner * below
        small = jnp.where(near, n_mat, 0.0)
        parts = split(small)
        square = passes(parts, diagonal(parts))
        yield
        halves = split(square)
        spread2 = diagonal(halves)
        fourth = passes(halves, spread2)
        yield
        start = eye - small + square - passes(parts, spread2)
        yield
        solved = start + passes(split(start), diagonal(split(fourth)))
        yield
        own = split(solved)
        spread_own = diagonal(own)
        lower = jnp.where(near, 0.0, n_mat)
        first_power = passes(own, diagonal(split(lower)))
        right = jnp.concatenate([keys * column(2, s), v_ref[s] * column(0, s)], axis=1)
        softened = passes(spread_own, split(right))
        yield
        parts = split(first_power)
        square = passes(parts, diagonal(parts))
        yield
        halves = split(square)
        spread2 = diagonal(halves)
        fourth = passes(halves, spread2)
        start = eye - first_power + square - passes(parts, spread2)
        yield
        chain8 = start + passes(split(start), diagonal(split(fourth)))
        yield
        deltas = passes(diagonal(split(chain8)), split(softened))
        yield
        kept = keys * column(3, s)
        turned = jnp.transpose(deltas)
        pairs = []
        for p in range(blocks // 2):
            cut = slice(2 * p * BLOCK, 2 * (p + 1) * BLOCK)
            spans = jnp.concatenate(
                [jnp.where(row_b[cut] == 2 * p + b, kept[cut], 0.0) for b in range(2)], axis=1
            )
            pairs.append(product(turned[:, cut], spans))
        yield
        moved = jnp.concatenate(pairs, axis=1)
        pieces = []
        for b in range(blocks):
            decay = jnp.exp(total[s : s + 1, b * BLOCK : b * BLOCK + 1])
            part = moved[:, b * head : (b + 1) * head]
            pieces.append((decay * head_eye - part[:head], part[head:]))
        while len(pieces) > 1:
            merged = []
            for early, late in zip(pieces[0::2], pieces[1::2]):
                both = product(jnp.concatenate(early, axis=0), late[0])
                merged.append((both[:head], both[head:] + late[1]))
            pieces = merged
            yield
        ab_ref[s, 0], ab_ref[s, 1] = pieces[0]
        yield

    for _ in zip(*[solve(s) for s in range(seqs)]):
        pass

    def chain(s, half):
        return pltpu.make_async_remote_copy(
            src_ref=tx_ref.at[s, half],
            dst_ref=rx_ref.at[s, half],
            send_sem=send_x.at[s, half],
            recv_sem=recv_x.at[s, half],
            device_id=at(lax.rem(me + 1, count)),
            device_id_type=MESH,
        )

    def push(s):
        return pltpu.make_async_remote_copy(
            src_ref=ab_ref.at[s, 1],
            dst_ref=first_ref.at[s],
            send_sem=send_f.at[s],
            recv_sem=recv_f.at[s],
            device_id=at(last_one),
            device_id_type=MESH,
        )

    decoded = pltpu.make_async_remote_copy(
        src_ref=new_tx,
        dst_ref=new_rx,
        send_sem=send_n,
        recv_sem=recv_n,
        device_id=at(last_one),
        device_id_type=MESH,
    )

    def rows_to(s, k):
        to = lax.rem(me + k, count)
        return pltpu.make_async_remote_copy(
            src_ref=out_tx.at[s, to],
            dst_ref=out_rx.at[s],
            send_sem=send_o.at[s, k],
            recv_sem=recv_o.at[s],
            device_id=at(to),
            device_id_type=MESH,
        )

    @pl.when(is_first)
    def _():
        pl.semaphore_wait(barrier, 1)
        for s in range(seqs):
            push(s).start()

    @pl.when(in_chain)
    def _():
        pl.semaphore_wait(barrier, 1)
        for half in range(2):
            for s in range(seqs):

                @pl.when(is_second)
                def _():
                    tx_ref[s, half] = ab_ref[s, half]

                @pl.when(jnp.logical_not(is_second))
                def _():
                    chain(s, half).wait_recv()
                    moved = product(rx_ref[s, half], ab_ref[s, 0])
                    tx_ref[s, half] = moved + ab_ref[s, 1] if half else moved

                chain(s, half).start()

    @pl.when(is_decoder)
    def _():
        for copy in load_dec:
            copy.wait()
        dec = dec_ref[...]
        new_kv = silu(dot(dec, wkv_ref[...]))
        new_key = unit_rows(new_kv[:, :head])
        new_value = new_kv[:, head:]
        query = silu(dot(dec, wq_ref[...]))
        both = dot_nt(gate_ref[...], dec)
        row_n = iota((gates, seqs), 0)
        picked = [
            jnp.sum(jnp.where(row_n == local_head, part, 0.0), axis=0, keepdims=True)
            for part in (both[:gates], both[gates:])
        ]
        new_beta = jax.nn.sigmoid(picked[0] - write_offset)
        keep = jnp.exp(-rate * softplus(picked[1]))
        for s in range(seqs):
            one = slice(s, s + 1)
            new_tx[s, 0:1] = new_key[one]
            new_tx[s, 1:2] = query[one]
            new_tx[s, 2:3] = new_value[one]
            new_tx[s, 3:4] = jnp.broadcast_to(new_beta[:, one], (1, head))
            new_tx[s, 4:5] = jnp.broadcast_to(keep[:, one], (1, head))
            new_tx[s, 5:8] = jnp.zeros((3, head), F32)
        decoded.start()

    @pl.when(is_last)
    def _():
        pl.semaphore_wait(barrier, count - 1)
        load_r.wait()
        joins = []
        for s in range(seqs):
            chain(s, 0).wait_recv()
            push(s).wait_recv()
            joins.append(product(first_ref[s], rx_ref[s, 0]))
        decoded.wait_recv()
        ahead = []
        for s in range(seqs):
            step, own = split(ab_ref[s, 0]), ab_ref[s, 1]
            new = split(new_rx[s])
            read_step = passes(new, step, dot_nt)
            ahead.append((step, split(read_step), passes(new, split(own), dot_nt)))
        for s in range(seqs):
            step, read_step, read_own = ahead[s]
            chain(s, 1).wait_recv()
            joined = split(joins[s] + rx_ref[s, 1])
            flipped = passes(joined, step) + ab_ref[s, 1]
            reads = passes(read_step, joined, dot_nt) + read_own
            new = new_rx[s]
            final = jnp.transpose(flipped)
            key_read, query_read = reads[0:1], reads[1:2]
            value, beta, hold = new[2:3], new[3:4], new[4:5]
            inter = jnp.sum(new[0:1] * new[1:2], axis=-1, keepdims=True)
            key_col = jnp.transpose(new)[:, 0:1]
            cache = hold * final + key_col * (beta * value - (hold * beta) * key_read)
            mixed = hold * query_read - (hold * beta * inter) * key_read + (beta * inter) * value
            scale = lax.rsqrt(jnp.sum(mixed * mixed, axis=-1, keepdims=True) / head + epsilon)
            read = mixed * scale * gain_ref[...]
            each = head // count
            out_tx[s, :, :each] = cache.reshape(count, each, head)
            out_tx[s, :, each:] = jnp.broadcast_to(read.reshape(1, 1, head), (count, each, head))
            for k in range(1, count):
                rows_to(s, k).start()
            out_rx[s] = out_tx[s, last_one]

    for s in range(seqs):

        @pl.when(jnp.logical_not(is_last))
        def _():
            rows_to(s, 1).wait_recv()

        each = head // count
        cache_ref[s, 0] = out_rx[s, :each].astype(BF16)
        read_ref[s : s + 1] = out_rx[s, each : each + 1].astype(BF16)

    @pl.when(jnp.logical_not(is_last))
    def _():
        load_r.wait()

    @pl.when(is_first)
    def _():
        for s in range(seqs):
            push(s).wait_send()

    @pl.when(is_decoder)
    def _():
        decoded.wait_send()

    @pl.when(in_chain)
    def _():
        for half in range(2):
            for s in range(seqs):
                chain(s, half).wait_send()

    @pl.when(is_last)
    def _():
        for s in range(seqs):
            for k in range(1, count):
                rows_to(s, k).wait_send()


def per_device(
    tokens,
    decoded_input,
    query_weight,
    key_weight,
    value_weight,
    gate_weight,
    head_decay_rate,
    extra_log_decay,
    read_norm_gain,
):
    seqs, rows, width = tokens.shape
    head = key_weight.shape[1]
    count = lax.axis_size("sp")
    each = head // count
    gates = gate_weight.transpose(1, 2, 0).reshape(-1, width)
    vmem = pl.BlockSpec(memory_space=pltpu.VMEM)
    hbm = pl.BlockSpec(memory_space=pltpu.HBM)
    dma = pltpu.SemaphoreType.DMA
    return pl.pallas_call(
        functools.partial(kernel, seqs, rows, count),
        out_shape=(
            jax.ShapeDtypeStruct((seqs, 1, each, head), BF16),
            jax.ShapeDtypeStruct((seqs, head), BF16),
        ),
        in_specs=[hbm] * 9,
        out_specs=(vmem, vmem),
        scratch_shapes=[
            pltpu.VMEM((seqs, rows, width), BF16),
            pltpu.VMEM((seqs, width), BF16),
            pltpu.VMEM((width, 2 * head), BF16),
            pltpu.VMEM((width, head), BF16),
            pltpu.VMEM((2 * GROUP, width), BF16),
            pltpu.SMEM((1,), F32),
            pltpu.VMEM((seqs, 1, rows), F32),
            pltpu.VMEM((1, head), F32),
            pltpu.VMEM((seqs, rows, head), F32),
            pltpu.VMEM((seqs, rows, head), F32),
            pltpu.VMEM((seqs, 2, head, head), F32),
            pltpu.VMEM((seqs, 2, head, head), F32),
            pltpu.VMEM((seqs, 2, head, head), F32),
            pltpu.VMEM((seqs, head, head), F32),
            pltpu.VMEM((seqs, 8, head), F32),
            pltpu.VMEM((seqs, 8, head), F32),
            pltpu.VMEM((seqs, count, 2 * each, head), F32),
            pltpu.VMEM((seqs, 2 * each, head), F32),
            dma((8 + CHUNKS * (seqs + 4),)),
            dma((seqs, 2)),
            dma((seqs, 2)),
            dma((seqs,)),
            dma((seqs,)),
            dma,
            dma,
            dma((seqs, count)),
            dma((seqs,)),
        ],
        compiler_params=pltpu.CompilerParams(
            collective_id=0, has_side_effects=True, vmem_limit_bytes=GRANT
        ),
    )(*[x if x.shape == (1,) else pltpu.with_memory_space_constraint(x, pltpu.HBM) for x in (
        tokens,
        decoded_input,
        query_weight,
        key_weight,
        value_weight,
        gates,
        head_decay_rate,
        extra_log_decay,
        read_norm_gain.reshape(1, head),
    )]    )


def solution(mesh):
    in_specs = (
        P("grp", "sp", None),
        P("grp", None),
        P(None, "tp"),
        P(None, "tp"),
        P(None, "tp"),
        P(),
        P("tp"),
        P("grp", "tp", "sp"),
        P(),
    )
    out_specs = (P("grp", "tp", "sp", None), P("grp", "tp"))
    return jax.shard_map(
        per_device, mesh=mesh, in_specs=in_specs, out_specs=out_specs, check_vma=False
    )
```

```python
import functools

import jax
import jax.numpy as jnp
from jax import lax
from jax.experimental import pallas as pl
from jax.experimental.pallas import tpu as pltpu
from jax.sharding import PartitionSpec as P

MESH = pl.DeviceIdType.MESH
F32 = jnp.float32
BF16 = jnp.bfloat16
epsilon = 1e-06
write_offset = 5.0
BLOCK = 64
CHUNKS = 4
NEAR = 3
GROUP = 8
GRANT = 24 << 20


def split(x):
    hi = x.astype(BF16)
    lo = (x - hi.astype(F32)).astype(BF16)
    return hi, lo


def dot(a, b):
    return jnp.dot(a, b, preferred_element_type=F32)


def dot_nt(a, b):
    return lax.dot_general(a, b, (((1,), (1,)), ((), ())), preferred_element_type=F32)


def passes(a, b, one=dot):
    if a[0].shape[1] == 128:
        wide = jnp.concatenate(a, axis=1)
        twice = jnp.concatenate([b[0], b[0]], axis=0 if one is dot else 1)
        return one(wide, twice) + one(a[0], b[1])
    rows = a[0].shape[0]
    both = one(jnp.concatenate([a[0], a[1]], axis=0), b[0])
    return both[:rows] + (one(a[0], b[1]) + both[rows:])


def product(a, b, one=dot):
    return passes(split(a), split(b), one)


def silu(x):
    return x * jax.nn.sigmoid(x)


def softplus(x):
    return jnp.maximum(x, 0.0) + jnp.log1p(jnp.exp(-jnp.abs(x)))


def unit_rows(x):
    return x * lax.rsqrt(jnp.sum(x * x, axis=-1, keepdims=True) + epsilon)


def iota(shape, dim):
    return lax.broadcasted_iota(jnp.int32, shape, dim)


def kernel(
    seqs,
    rows,
    count,
    tok_hbm,
    dec_hbm,
    wq_hbm,
    wk_hbm,
    wv_hbm,
    gate_hbm,
    rate_hbm,
    extra_hbm,
    gain_hbm,
    cache_ref,
    read_ref,
    x_ref,
    dec_ref,
    wkv_ref,
    wq_ref,
    gate_ref,
    rate_ref,
    extra_ref,
    gain_ref,
    k_ref,
    v_ref,
    ab_ref,
    rx_ref,
    tx_ref,
    first_ref,
    new_tx,
    new_rx,
    out_tx,
    out_rx,
    load_sem,
    send_x,
    recv_x,
    send_f,
    recv_f,
    send_n,
    recv_n,
    send_o,
    recv_o,
):
    me = lax.axis_index("sp")
    head_index = lax.axis_index("tp")
    head = k_ref.shape[-1]
    gates = GROUP
    heads = gate_hbm.shape[0] // 2
    first = pl.multiple_of(head_index // GROUP * GROUP, GROUP)
    local_head = lax.rem(head_index, GROUP)
    last_one = count - 1
    is_first = me == 0
    is_second = me == 1
    is_decoder = me == 0
    is_last = me == last_one
    in_chain = jnp.logical_and(me > 0, me < last_one)

    def load(source, target, place):
        copy = pltpu.make_async_copy(source, target, load_sem.at[place])
        copy.start()
        return copy

    width = x_ref.shape[-1]
    wide = width // CHUNKS
    loads = []
    for c in range(CHUNKS):
        cut = pl.ds(c * wide, wide)
        pairs = [
            (wk_hbm.at[cut], wkv_ref.at[cut, pl.ds(0, head)]),
            (wv_hbm.at[cut], wkv_ref.at[cut, pl.ds(head, head)]),
        ]
        pairs += [(tok_hbm.at[s, :, cut], x_ref.at[s, :, cut]) for s in range(seqs)]
        pairs += [
            (gate_hbm.at[pl.ds(first + g // GROUP * heads, GROUP), cut], gate_ref.at[pl.ds(g, GROUP), cut])
            for g in (0, GROUP)
        ]
        loads.append(
            [load(pair[0], pair[1], 8 + c * len(pairs) + i) for i, pair in enumerate(pairs)]
        )
    load_g = [load(rate_hbm, rate_ref, 4), load(extra_hbm, extra_ref, 5)]
    load_r = load(gain_hbm, gain_ref, 6)
    load_dec = [
        pltpu.make_async_copy(dec_hbm, dec_ref, load_sem.at[7]),
        pltpu.make_async_copy(wq_hbm, wq_ref, load_sem.at[3]),
    ]

    @pl.when(is_decoder)
    def _():
        for copy in load_dec:
            copy.start()


    def at(index):
        return {"sp": index}

    barrier = pltpu.get_barrier_semaphore()

    def greet(index):
        pl.semaphore_signal(barrier, inc=1, device_id=at(index), device_id_type=MESH)

    @pl.when(me >= 2)
    def _():
        greet(me - 1)

    @pl.when(is_last)
    def _():
        greet(0)

    @pl.when(jnp.logical_not(is_last))
    def _():
        greet(last_one)

    row_g = iota((gates, rows), 0)
    sums = [None] * seqs
    gate_sums = [None] * seqs
    for c in range(CHUNKS):
        for copy in loads[c]:
            copy.wait()
        cut = slice(c * wide, (c + 1) * wide)
        for s in range(seqs):
            part = dot(x_ref[s, :, cut], wkv_ref[cut])
            sums[s] = part if c == 0 else sums[s] + part
            part = dot_nt(gate_ref[:, cut], x_ref[s, :, cut])
            gate_sums[s] = part if c == 0 else gate_sums[s] + part
    for copy in load_g:
        copy.wait()
    gate_rows = []
    for s in range(seqs):
        kv = silu(sums[s])
        k_ref[s] = unit_rows(kv[:, :head])
        v_ref[s] = kv[:, head:]
        picked = [
            jnp.sum(jnp.where(row_g == local_head, part, 0.0), axis=0, keepdims=True)
            for part in (gate_sums[s][:gates], gate_sums[s][gates:])
        ]
        gate_rows.append(picked)
    rate = rate_ref[0]
    betas = [jax.nn.sigmoid(g[0] - write_offset) for g in gate_rows]
    decays = [-rate * softplus(g[1]) + extra_ref[s] for s, g in enumerate(gate_rows)]
    stacked = jnp.concatenate(decays, axis=0)
    hi, rest = split(stacked)
    rest32 = stacked - hi.astype(F32)
    lo = (rest32 - rest.astype(F32)).astype(BF16)
    parts = (hi, rest, lo)
    row_i = iota((rows, rows), 0)
    col_i = iota((rows, rows), 1)
    together = row_i // BLOCK == col_i // BLOCK
    upto = jnp.where(jnp.logical_and(together, row_i <= col_i), 1.0, 0.0).astype(BF16)
    whole = jnp.where(together, 1.0, 0.0).astype(BF16)
    running = sum(dot(part, upto) for part in parts)
    total = sum(dot(part, whole) for part in parts)
    grown = jnp.exp(running)
    packed = jnp.concatenate(
        betas
        + [running]
        + [betas[s] * grown[s : s + 1] for s in range(seqs)]
        + [jnp.exp(total - running)],
        axis=0,
    )
    columns = jnp.transpose(packed)

    def column(kind, s):
        place = kind * seqs + s
        return columns[:, place : place + 1]

    blocks = rows // BLOCK
    row_c = iota((BLOCK, rows), 0)
    lane_c = iota((BLOCK, rows), 1)
    inside = lax.bitwise_and(lane_c, BLOCK - 1)
    owner = lane_c // BLOCK
    own_lanes = [owner == b for b in range(blocks)]
    strict = row_c > inside
    eye = jnp.where(row_c == inside, 1.0, 0.0)

    def compact(full):
        out = jnp.where(owner == 0, full[:BLOCK], 0.0)
        for b in range(1, blocks):
            out = jnp.where(owner == b, full[b * BLOCK : (b + 1) * BLOCK], out)
        return out

    def diagonal(pair):
        return [jnp.concatenate([jnp.where(own, part, jnp.zeros_like(part)) for own in own_lanes], axis=0) for part in pair]

    head_eye = jnp.where(iota((head, head), 0) == iota((head, head), 1), 1.0, 0.0)
    row_b = iota((rows, 1), 0) // BLOCK
    near = row_c // 8 == inside // 8

    def solve(s):
        keys = k_ref[s]
        halves = split(keys)
        inner = compact(passes(halves, halves, dot_nt))
        yield
        spread = compact(jnp.broadcast_to(column(1, s), (rows, rows))) - running[s : s + 1]
        below = jnp.where(strict, jnp.exp(jnp.where(strict, spread, 0.0)), 0.0)
        yield
        n_mat = compact(jnp.broadcast_to(column(0, s), (rows, rows))) * inner * below
        small = jnp.where(near, n_mat, 0.0)
        parts = split(small)
        square = passes(parts, diagonal(parts))
        yield
        halves = split(square)
        spread2 = diagonal(halves)
        fourth = passes(halves, spread2)
        yield
        start = eye - small + square - passes(parts, spread2)
        yield
        solved = start + passes(split(start), diagonal(split(fourth)))
        yield
        own = split(solved)
        spread_own = diagonal(own)
        lower = jnp.where(near, 0.0, n_mat)
        first_power = passes(own, diagonal(split(lower)))
        right = jnp.concatenate([keys * column(2, s), v_ref[s] * column(0, s)], axis=1)
        softened = passes(spread_own, split(right))
        yield
        parts = split(first_power)
        square = passes(parts, diagonal(parts))
        yield
        halves = split(square)
        spread2 = diagonal(halves)
        fourth = passes(halves, spread2)
        start = eye - first_power + square - passes(parts, spread2)
        yield
        chain8 = start + passes(split(start), diagonal(split(fourth)))
        yield
        deltas = passes(diagonal(split(chain8)), split(softened))
        yield
        kept = keys * column(3, s)
        turned = jnp.transpose(deltas)
        pairs = []
        for p in range(blocks // 2):
            cut = slice(2 * p * BLOCK, 2 * (p + 1) * BLOCK)
            spans = jnp.concatenate(
                [jnp.where(row_b[cut] == 2 * p + b, kept[cut], 0.0) for b in range(2)], axis=1
            )
            pairs.append(product(turned[:, cut], spans))
        yield
        moved = jnp.concatenate(pairs, axis=1)
        pieces = []
        for b in range(blocks):
            decay = jnp.exp(total[s : s + 1, b * BLOCK : b * BLOCK + 1])
            part = moved[:, b * head : (b + 1) * head]
            pieces.append((decay * head_eye - part[:head], part[head:]))
        while len(pieces) > 1:
            merged = []
            for early, late in zip(pieces[0::2], pieces[1::2]):
                both = product(jnp.concatenate(early, axis=0), late[0])
                merged.append((both[:head], both[head:] + late[1]))
            pieces = merged
            yield
        ab_ref[s, 0], ab_ref[s, 1] = pieces[0]
        yield

    for _ in zip(*[solve(s) for s in range(seqs)]):
        pass

    def chain(s, half):
        return pltpu.make_async_remote_copy(
            src_ref=tx_ref.at[s, half],
            dst_ref=rx_ref.at[s, half],
            send_sem=send_x.at[s, half],
            recv_sem=recv_x.at[s, half],
            device_id=at(lax.rem(me + 1, count)),
            device_id_type=MESH,
        )

    def push(s):
        return pltpu.make_async_remote_copy(
            src_ref=ab_ref.at[s, 1],
            dst_ref=first_ref.at[s],
            send_sem=send_f.at[s],
            recv_sem=recv_f.at[s],
            device_id=at(last_one),
            device_id_type=MESH,
        )

    decoded = pltpu.make_async_remote_copy(
        src_ref=new_tx,
        dst_ref=new_rx,
        send_sem=send_n,
        recv_sem=recv_n,
        device_id=at(last_one),
        device_id_type=MESH,
    )

    def rows_to(s, k):
        to = lax.rem(me + k, count)
        return pltpu.make_async_remote_copy(
            src_ref=out_tx.at[s, to],
            dst_ref=out_rx.at[s],
            send_sem=send_o.at[s, k],
            recv_sem=recv_o.at[s],
            device_id=at(to),
            device_id_type=MESH,
        )

    @pl.when(is_first)
    def _():
        pl.semaphore_wait(barrier, 1)
        for s in range(seqs):
            push(s).start()

    @pl.when(in_chain)
    def _():
        pl.semaphore_wait(barrier, 1)
        for half in range(2):
            for s in range(seqs):

                @pl.when(is_second)
                def _():
                    tx_ref[s, half] = ab_ref[s, half]

                @pl.when(jnp.logical_not(is_second))
                def _():
                    chain(s, half).wait_recv()
                    moved = product(rx_ref[s, half], ab_ref[s, 0])
                    tx_ref[s, half] = moved + ab_ref[s, 1] if half else moved

                chain(s, half).start()

    @pl.when(is_decoder)
    def _():
        for copy in load_dec:
            copy.wait()
        dec = dec_ref[...]
        new_kv = silu(dot(dec, wkv_ref[...]))
        new_key = unit_rows(new_kv[:, :head])
        new_value = new_kv[:, head:]
        query = silu(dot(dec, wq_ref[...]))
        both = dot_nt(gate_ref[...], dec)
        row_n = iota((gates, seqs), 0)
        picked = [
            jnp.sum(jnp.where(row_n == local_head, part, 0.0), axis=0, keepdims=True)
            for part in (both[:gates], both[gates:])
        ]
        new_beta = jax.nn.sigmoid(picked[0] - write_offset)
        keep = jnp.exp(-rate * softplus(picked[1]))
        for s in range(seqs):
            one = slice(s, s + 1)
            new_tx[s, 0:1] = new_key[one]
            new_tx[s, 1:2] = query[one]
            new_tx[s, 2:3] = new_value[one]
            new_tx[s, 3:4] = jnp.broadcast_to(new_beta[:, one], (1, head))
            new_tx[s, 4:5] = jnp.broadcast_to(keep[:, one], (1, head))
            new_tx[s, 5:8] = jnp.zeros((3, head), F32)
        decoded.start()

    @pl.when(is_last)
    def _():
        pl.semaphore_wait(barrier, count - 1)
        load_r.wait()
        joins = []
        for s in range(seqs):
            chain(s, 0).wait_recv()
            push(s).wait_recv()
            joins.append(product(first_ref[s], rx_ref[s, 0]))
        decoded.wait_recv()
        ahead = []
        for s in range(seqs):
            step, own = split(ab_ref[s, 0]), ab_ref[s, 1]
            new = split(new_rx[s])
            read_step = passes(new, step, dot_nt)
            ahead.append((step, split(read_step), passes(new, split(own), dot_nt)))
        for s in range(seqs):
            step, read_step, read_own = ahead[s]
            chain(s, 1).wait_recv()
            joined = split(joins[s] + rx_ref[s, 1])
            flipped = passes(joined, step) + ab_ref[s, 1]
            reads = passes(read_step, joined, dot_nt) + read_own
            new = new_rx[s]
            final = jnp.transpose(flipped)
            key_read, query_read = reads[0:1], reads[1:2]
            value, beta, hold = new[2:3], new[3:4], new[4:5]
            inter = jnp.sum(new[0:1] * new[1:2], axis=-1, keepdims=True)
            key_col = jnp.transpose(new)[:, 0:1]
            cache = hold * final + key_col * (beta * value - (hold * beta) * key_read)
            mixed = hold * query_read - (hold * beta * inter) * key_read + (beta * inter) * value
            scale = lax.rsqrt(jnp.sum(mixed * mixed, axis=-1, keepdims=True) / head + epsilon)
            read = mixed * scale * gain_ref[...]
            each = head // count
            out_tx[s, :, :each] = cache.reshape(count, each, head)
            out_tx[s, :, each:] = jnp.broadcast_to(read.reshape(1, 1, head), (count, each, head))
            for k in range(1, NEAR):
                rows_to(s, k).start()
            out_rx[s] = out_tx[s, last_one]
        for s in range(seqs):
            for k in range(NEAR, count):
                rows_to(s, k).start()

    for s in range(seqs):

        @pl.when(jnp.logical_not(is_last))
        def _():
            rows_to(s, 1).wait_recv()

        each = head // count
        cache_ref[s, 0] = out_rx[s, :each].astype(BF16)
        read_ref[s : s + 1] = out_rx[s, each : each + 1].astype(BF16)

    @pl.when(jnp.logical_not(is_last))
    def _():
        load_r.wait()

    @pl.when(is_first)
    def _():
        for s in range(seqs):
            push(s).wait_send()

    @pl.when(is_decoder)
    def _():
        decoded.wait_send()

    @pl.when(in_chain)
    def _():
        for half in range(2):
            for s in range(seqs):
                chain(s, half).wait_send()

    @pl.when(is_last)
    def _():
        for s in range(seqs):
            for k in range(1, count):
                rows_to(s, k).wait_send()


def per_device(
    tokens,
    decoded_input,
    query_weight,
    key_weight,
    value_weight,
    gate_weight,
    head_decay_rate,
    extra_log_decay,
    read_norm_gain,
):
    seqs, rows, width = tokens.shape
    head = key_weight.shape[1]
    count = lax.axis_size("sp")
    each = head // count
    gates = gate_weight.transpose(1, 2, 0).reshape(-1, width)
    vmem = pl.BlockSpec(memory_space=pltpu.VMEM)
    hbm = pl.BlockSpec(memory_space=pltpu.HBM)
    dma = pltpu.SemaphoreType.DMA
    return pl.pallas_call(
        functools.partial(kernel, seqs, rows, count),
        out_shape=(
            jax.ShapeDtypeStruct((seqs, 1, each, head), BF16),
            jax.ShapeDtypeStruct((seqs, head), BF16),
        ),
        in_specs=[hbm] * 9,
        out_specs=(vmem, vmem),
        scratch_shapes=[
            pltpu.VMEM((seqs, rows, width), BF16),
            pltpu.VMEM((seqs, width), BF16),
            pltpu.VMEM((width, 2 * head), BF16),
            pltpu.VMEM((width, head), BF16),
            pltpu.VMEM((2 * GROUP, width), BF16),
            pltpu.SMEM((1,), F32),
            pltpu.VMEM((seqs, 1, rows), F32),
            pltpu.VMEM((1, head), F32),
            pltpu.VMEM((seqs, rows, head), F32),
            pltpu.VMEM((seqs, rows, head), F32),
            pltpu.VMEM((seqs, 2, head, head), F32),
            pltpu.VMEM((seqs, 2, head, head), F32),
            pltpu.VMEM((seqs, 2, head, head), F32),
            pltpu.VMEM((seqs, head, head), F32),
            pltpu.VMEM((seqs, 8, head), F32),
            pltpu.VMEM((seqs, 8, head), F32),
            pltpu.VMEM((seqs, count, 2 * each, head), F32),
            pltpu.VMEM((seqs, 2 * each, head), F32),
            dma((8 + CHUNKS * (seqs + 4),)),
            dma((seqs, 2)),
            dma((seqs, 2)),
            dma((seqs,)),
            dma((seqs,)),
            dma,
            dma,
            dma((seqs, count)),
            dma((seqs,)),
        ],
        compiler_params=pltpu.CompilerParams(
            collective_id=0, has_side_effects=True, vmem_limit_bytes=GRANT
        ),
    )(*[x if x.shape == (1,) else pltpu.with_memory_space_constraint(x, pltpu.HBM) for x in (
        tokens,
        decoded_input,
        query_weight,
        key_weight,
        value_weight,
        gates,
        head_decay_rate,
        extra_log_decay,
        read_norm_gain.reshape(1, head),
    )]    )


def solution(mesh):
    in_specs = (
        P("grp", "sp", None),
        P("grp", None),
        P(None, "tp"),
        P(None, "tp"),
        P(None, "tp"),
        P(),
        P("tp"),
        P("grp", "tp", "sp"),
        P(),
    )
    out_specs = (P("grp", "tp", "sp", None), P("grp", "tp"))
    return jax.shard_map(
        per_device, mesh=mesh, in_specs=in_specs, out_specs=out_specs, check_vma=False
    )
```

```python
import functools

import jax
import jax.numpy as jnp
from jax import lax
from jax.experimental import pallas as pl
from jax.experimental.pallas import tpu as pltpu
from jax.sharding import PartitionSpec as P

MESH = pl.DeviceIdType.MESH
F32 = jnp.float32
BF16 = jnp.bfloat16
epsilon = 1e-06
write_offset = 5.0
BLOCK = 64
CHUNKS = 4
NEAR = 3
GROUP = 8
GRANT = 24 << 20


def split(x):
    hi = x.astype(BF16)
    lo = (x - hi.astype(F32)).astype(BF16)
    return hi, lo


def dot(a, b):
    return jnp.dot(a, b, preferred_element_type=F32)


def dot_nt(a, b):
    return lax.dot_general(a, b, (((1,), (1,)), ((), ())), preferred_element_type=F32)


def passes(a, b, one=dot):
    if a[0].shape[1] == 128:
        wide = jnp.concatenate(a, axis=1)
        twice = jnp.concatenate([b[0], b[0]], axis=0 if one is dot else 1)
        return one(wide, twice) + one(a[0], b[1])
    rows = a[0].shape[0]
    both = one(jnp.concatenate([a[0], a[1]], axis=0), b[0])
    return both[:rows] + (one(a[0], b[1]) + both[rows:])


def product(a, b, one=dot):
    return passes(split(a), split(b), one)


def silu(x):
    return x * jax.nn.sigmoid(x)


def softplus(x):
    return jnp.maximum(x, 0.0) + jnp.log1p(jnp.exp(-jnp.abs(x)))


def unit_rows(x):
    return x * lax.rsqrt(jnp.sum(x * x, axis=-1, keepdims=True) + epsilon)


def iota(shape, dim):
    return lax.broadcasted_iota(jnp.int32, shape, dim)


def kernel(
    seqs,
    rows,
    count,
    tok_hbm,
    dec_hbm,
    wq_hbm,
    wk_hbm,
    wv_hbm,
    gate_hbm,
    rate_hbm,
    extra_hbm,
    gain_hbm,
    cache_ref,
    read_ref,
    x_ref,
    dec_ref,
    wkv_ref,
    wq_ref,
    gate_ref,
    rate_ref,
    extra_ref,
    gain_ref,
    k_ref,
    v_ref,
    ab_ref,
    rx_ref,
    tx_ref,
    first_ref,
    new_tx,
    new_rx,
    out_tx,
    out_rx,
    load_sem,
    send_x,
    recv_x,
    send_f,
    recv_f,
    send_n,
    recv_n,
    send_o,
    recv_o,
):
    me = lax.axis_index("sp")
    head_index = lax.axis_index("tp")
    head = k_ref.shape[-1]
    gates = GROUP
    heads = gate_hbm.shape[0] // 2
    first = pl.multiple_of(head_index // GROUP * GROUP, GROUP)
    local_head = lax.rem(head_index, GROUP)
    last_one = count - 1
    is_first = me == 0
    is_second = me == 1
    goes_first = lax.rem(head_index, 2) == 0
    is_decoder = me == 0
    is_last = me == last_one
    in_chain = jnp.logical_and(me > 0, me < last_one)

    def load(source, target, place):
        copy = pltpu.make_async_copy(source, target, load_sem.at[place])
        copy.start()
        return copy

    width = x_ref.shape[-1]
    wide = width // CHUNKS
    loads = []
    for c in range(CHUNKS):
        cut = pl.ds(c * wide, wide)
        pairs = [
            (wk_hbm.at[cut], wkv_ref.at[cut, pl.ds(0, head)]),
            (wv_hbm.at[cut], wkv_ref.at[cut, pl.ds(head, head)]),
        ]
        pairs += [(tok_hbm.at[s, :, cut], x_ref.at[s, :, cut]) for s in range(seqs)]
        pairs += [
            (gate_hbm.at[pl.ds(first + g // GROUP * heads, GROUP), cut], gate_ref.at[pl.ds(g, GROUP), cut])
            for g in (0, GROUP)
        ]
        loads.append(
            [load(pair[0], pair[1], 8 + c * len(pairs) + i) for i, pair in enumerate(pairs)]
        )
    load_g = [load(rate_hbm, rate_ref, 4), load(extra_hbm, extra_ref, 5)]
    load_r = load(gain_hbm, gain_ref, 6)
    load_dec = [
        pltpu.make_async_copy(dec_hbm, dec_ref, load_sem.at[7]),
        pltpu.make_async_copy(wq_hbm, wq_ref, load_sem.at[3]),
    ]

    @pl.when(is_decoder)
    def _():
        for copy in load_dec:
            copy.start()


    def at(index):
        return {"sp": index}

    barrier = pltpu.get_barrier_semaphore()

    def greet(index):
        pl.semaphore_signal(barrier, inc=1, device_id=at(index), device_id_type=MESH)

    @pl.when(me >= 2)
    def _():
        greet(me - 1)

    @pl.when(is_last)
    def _():
        greet(0)

    @pl.when(jnp.logical_not(is_last))
    def _():
        greet(last_one)

    row_g = iota((gates, rows), 0)
    sums = [None] * seqs
    gate_sums = [None] * seqs
    for c in range(CHUNKS):
        for copy in loads[c]:
            copy.wait()
        cut = slice(c * wide, (c + 1) * wide)
        for s in range(seqs):
            part = dot(x_ref[s, :, cut], wkv_ref[cut])
            sums[s] = part if c == 0 else sums[s] + part
            part = dot_nt(gate_ref[:, cut], x_ref[s, :, cut])
            gate_sums[s] = part if c == 0 else gate_sums[s] + part
    for copy in load_g:
        copy.wait()
    gate_rows = []
    for s in range(seqs):
        kv = silu(sums[s])
        k_ref[s] = unit_rows(kv[:, :head])
        v_ref[s] = kv[:, head:]
        picked = [
            jnp.sum(jnp.where(row_g == local_head, part, 0.0), axis=0, keepdims=True)
            for part in (gate_sums[s][:gates], gate_sums[s][gates:])
        ]
        gate_rows.append(picked)
    rate = rate_ref[0]
    betas = [jax.nn.sigmoid(g[0] - write_offset) for g in gate_rows]
    decays = [-rate * softplus(g[1]) + extra_ref[s] for s, g in enumerate(gate_rows)]
    stacked = jnp.concatenate(decays, axis=0)
    hi, rest = split(stacked)
    rest32 = stacked - hi.astype(F32)
    lo = (rest32 - rest.astype(F32)).astype(BF16)
    parts = (hi, rest, lo)
    row_i = iota((rows, rows), 0)
    col_i = iota((rows, rows), 1)
    together = row_i // BLOCK == col_i // BLOCK
    upto = jnp.where(jnp.logical_and(together, row_i <= col_i), 1.0, 0.0).astype(BF16)
    whole = jnp.where(together, 1.0, 0.0).astype(BF16)
    running = sum(dot(part, upto) for part in parts)
    total = sum(dot(part, whole) for part in parts)
    grown = jnp.exp(running)
    packed = jnp.concatenate(
        betas
        + [running]
        + [betas[s] * grown[s : s + 1] for s in range(seqs)]
        + [jnp.exp(total - running)],
        axis=0,
    )
    columns = jnp.transpose(packed)

    def column(kind, s):
        place = kind * seqs + s
        return columns[:, place : place + 1]

    blocks = rows // BLOCK
    row_c = iota((BLOCK, rows), 0)
    lane_c = iota((BLOCK, rows), 1)
    inside = lax.bitwise_and(lane_c, BLOCK - 1)
    owner = lane_c // BLOCK
    own_lanes = [owner == b for b in range(blocks)]
    strict = row_c > inside
    eye = jnp.where(row_c == inside, 1.0, 0.0)

    def compact(full):
        out = jnp.where(owner == 0, full[:BLOCK], 0.0)
        for b in range(1, blocks):
            out = jnp.where(owner == b, full[b * BLOCK : (b + 1) * BLOCK], out)
        return out

    def diagonal(pair):
        return [jnp.concatenate([jnp.where(own, part, jnp.zeros_like(part)) for own in own_lanes], axis=0) for part in pair]

    head_eye = jnp.where(iota((head, head), 0) == iota((head, head), 1), 1.0, 0.0)
    row_b = iota((rows, 1), 0) // BLOCK
    near = row_c // 8 == inside // 8

    def solve(s):
        keys = k_ref[s]
        halves = split(keys)
        inner = compact(passes(halves, halves, dot_nt))
        yield
        spread = compact(jnp.broadcast_to(column(1, s), (rows, rows))) - running[s : s + 1]
        below = jnp.where(strict, jnp.exp(jnp.where(strict, spread, 0.0)), 0.0)
        yield
        n_mat = compact(jnp.broadcast_to(column(0, s), (rows, rows))) * inner * below
        small = jnp.where(near, n_mat, 0.0)
        parts = split(small)
        square = passes(parts, diagonal(parts))
        yield
        halves = split(square)
        spread2 = diagonal(halves)
        fourth = passes(halves, spread2)
        yield
        start = eye - small + square - passes(parts, spread2)
        yield
        solved = start + passes(split(start), diagonal(split(fourth)))
        yield
        own = split(solved)
        spread_own = diagonal(own)
        lower = jnp.where(near, 0.0, n_mat)
        first_power = passes(own, diagonal(split(lower)))
        right = jnp.concatenate([keys * column(2, s), v_ref[s] * column(0, s)], axis=1)
        softened = passes(spread_own, split(right))
        yield
        parts = split(first_power)
        square = passes(parts, diagonal(parts))
        yield
        halves = split(square)
        spread2 = diagonal(halves)
        fourth = passes(halves, spread2)
        start = eye - first_power + square - passes(parts, spread2)
        yield
        chain8 = start + passes(split(start), diagonal(split(fourth)))
        yield
        deltas = passes(diagonal(split(chain8)), split(softened))
        yield
        kept = keys * column(3, s)
        turned = jnp.transpose(deltas)
        pairs = []
        for p in range(blocks // 2):
            cut = slice(2 * p * BLOCK, 2 * (p + 1) * BLOCK)
            spans = jnp.concatenate(
                [jnp.where(row_b[cut] == 2 * p + b, kept[cut], 0.0) for b in range(2)], axis=1
            )
            pairs.append(product(turned[:, cut], spans))
        yield
        moved = jnp.concatenate(pairs, axis=1)
        pieces = []
        for b in range(blocks):
            decay = jnp.exp(total[s : s + 1, b * BLOCK : b * BLOCK + 1])
            part = moved[:, b * head : (b + 1) * head]
            pieces.append((decay * head_eye - part[:head], part[head:]))
        while len(pieces) > 1:
            merged = []
            for early, late in zip(pieces[0::2], pieces[1::2]):
                both = product(jnp.concatenate(early, axis=0), late[0])
                merged.append((both[:head], both[head:] + late[1]))
            pieces = merged
            yield
        ab_ref[s, 0], ab_ref[s, 1] = pieces[0]
        yield

    for _ in zip(*[solve(s) for s in range(seqs)]):
        pass

    def chain(s, half):
        return pltpu.make_async_remote_copy(
            src_ref=tx_ref.at[s, half],
            dst_ref=rx_ref.at[s, half],
            send_sem=send_x.at[s, half],
            recv_sem=recv_x.at[s, half],
            device_id=at(lax.rem(me + 1, count)),
            device_id_type=MESH,
        )

    def push(s):
        return pltpu.make_async_remote_copy(
            src_ref=ab_ref.at[s, 1],
            dst_ref=first_ref.at[s],
            send_sem=send_f.at[s],
            recv_sem=recv_f.at[s],
            device_id=at(last_one),
            device_id_type=MESH,
        )

    decoded = pltpu.make_async_remote_copy(
        src_ref=new_tx,
        dst_ref=new_rx,
        send_sem=send_n,
        recv_sem=recv_n,
        device_id=at(last_one),
        device_id_type=MESH,
    )

    def rows_to(s, k):
        to = lax.rem(me + k, count)
        return pltpu.make_async_remote_copy(
            src_ref=out_tx.at[s, to],
            dst_ref=out_rx.at[s],
            send_sem=send_o.at[s, k],
            recv_sem=recv_o.at[s],
            device_id=at(to),
            device_id_type=MESH,
        )

    @pl.when(is_first)
    def _():
        pl.semaphore_wait(barrier, 1)
        for s in range(seqs):
            push(s).start()

    @pl.when(in_chain)
    def _():
        pl.semaphore_wait(barrier, 1)
        for half in range(2):
            for s in range(seqs):

                @pl.when(is_second)
                def _():
                    tx_ref[s, half] = ab_ref[s, half]

                @pl.when(jnp.logical_not(is_second))
                def _():
                    chain(s, half).wait_recv()
                    moved = product(rx_ref[s, half], ab_ref[s, 0])
                    tx_ref[s, half] = moved + ab_ref[s, 1] if half else moved

                @pl.when(goes_first)
                def _():
                    chain(s, half).start()

            @pl.when(jnp.logical_not(goes_first))
            def _():
                for s in range(seqs):
                    chain(s, half).start()

    @pl.when(is_decoder)
    def _():
        for copy in load_dec:
            copy.wait()
        dec = dec_ref[...]
        new_kv = silu(dot(dec, wkv_ref[...]))
        new_key = unit_rows(new_kv[:, :head])
        new_value = new_kv[:, head:]
        query = silu(dot(dec, wq_ref[...]))
        both = dot_nt(gate_ref[...], dec)
        row_n = iota((gates, seqs), 0)
        picked = [
            jnp.sum(jnp.where(row_n == local_head, part, 0.0), axis=0, keepdims=True)
            for part in (both[:gates], both[gates:])
        ]
        new_beta = jax.nn.sigmoid(picked[0] - write_offset)
        keep = jnp.exp(-rate * softplus(picked[1]))
        for s in range(seqs):
            one = slice(s, s + 1)
            new_tx[s, 0:1] = new_key[one]
            new_tx[s, 1:2] = query[one]
            new_tx[s, 2:3] = new_value[one]
            new_tx[s, 3:4] = jnp.broadcast_to(new_beta[:, one], (1, head))
            new_tx[s, 4:5] = jnp.broadcast_to(keep[:, one], (1, head))
            new_tx[s, 5:8] = jnp.zeros((3, head), F32)
        decoded.start()

    @pl.when(is_last)
    def _():
        pl.semaphore_wait(barrier, count - 1)
        load_r.wait()
        joins = []
        for s in range(seqs):
            chain(s, 0).wait_recv()
            push(s).wait_recv()
            joins.append(product(first_ref[s], rx_ref[s, 0]))
        decoded.wait_recv()
        ahead = []
        for s in range(seqs):
            step, own = split(ab_ref[s, 0]), ab_ref[s, 1]
            new = split(new_rx[s])
            read_step = passes(new, step, dot_nt)
            ahead.append((step, split(read_step), passes(new, split(own), dot_nt)))
        for s in range(seqs):
            step, read_step, read_own = ahead[s]
            chain(s, 1).wait_recv()
            joined = split(joins[s] + rx_ref[s, 1])
            flipped = passes(joined, step) + ab_ref[s, 1]
            reads = passes(read_step, joined, dot_nt) + read_own
            new = new_rx[s]
            final = jnp.transpose(flipped)
            key_read, query_read = reads[0:1], reads[1:2]
            value, beta, hold = new[2:3], new[3:4], new[4:5]
            inter = jnp.sum(new[0:1] * new[1:2], axis=-1, keepdims=True)
            key_col = jnp.transpose(new)[:, 0:1]
            cache = hold * final + key_col * (beta * value - (hold * beta) * key_read)
            mixed = hold * query_read - (hold * beta * inter) * key_read + (beta * inter) * value
            scale = lax.rsqrt(jnp.sum(mixed * mixed, axis=-1, keepdims=True) / head + epsilon)
            read = mixed * scale * gain_ref[...]
            each = head // count
            out_tx[s, :, :each] = cache.reshape(count, each, head)
            out_tx[s, :, each:] = jnp.broadcast_to(read.reshape(1, 1, head), (count, each, head))
            for k in range(1, NEAR):
                rows_to(s, k).start()
            out_rx[s] = out_tx[s, last_one]
        for s in range(seqs):
            for k in range(NEAR, count):
                rows_to(s, k).start()

    for s in range(seqs):

        @pl.when(jnp.logical_not(is_last))
        def _():
            rows_to(s, 1).wait_recv()

        each = head // count
        cache_ref[s, 0] = out_rx[s, :each].astype(BF16)
        read_ref[s : s + 1] = out_rx[s, each : each + 1].astype(BF16)

    @pl.when(jnp.logical_not(is_last))
    def _():
        load_r.wait()

    @pl.when(is_first)
    def _():
        for s in range(seqs):
            push(s).wait_send()

    @pl.when(is_decoder)
    def _():
        decoded.wait_send()

    @pl.when(in_chain)
    def _():
        for half in range(2):
            for s in range(seqs):
                chain(s, half).wait_send()

    @pl.when(is_last)
    def _():
        for s in range(seqs):
            for k in range(1, count):
                rows_to(s, k).wait_send()


def per_device(
    tokens,
    decoded_input,
    query_weight,
    key_weight,
    value_weight,
    gate_weight,
    head_decay_rate,
    extra_log_decay,
    read_norm_gain,
):
    seqs, rows, width = tokens.shape
    head = key_weight.shape[1]
    count = lax.axis_size("sp")
    each = head // count
    gates = gate_weight.transpose(1, 2, 0).reshape(-1, width)
    vmem = pl.BlockSpec(memory_space=pltpu.VMEM)
    hbm = pl.BlockSpec(memory_space=pltpu.HBM)
    dma = pltpu.SemaphoreType.DMA
    return pl.pallas_call(
        functools.partial(kernel, seqs, rows, count),
        out_shape=(
            jax.ShapeDtypeStruct((seqs, 1, each, head), BF16),
            jax.ShapeDtypeStruct((seqs, head), BF16),
        ),
        in_specs=[hbm] * 9,
        out_specs=(vmem, vmem),
        scratch_shapes=[
            pltpu.VMEM((seqs, rows, width), BF16),
            pltpu.VMEM((seqs, width), BF16),
            pltpu.VMEM((width, 2 * head), BF16),
            pltpu.VMEM((width, head), BF16),
            pltpu.VMEM((2 * GROUP, width), BF16),
            pltpu.SMEM((1,), F32),
            pltpu.VMEM((seqs, 1, rows), F32),
            pltpu.VMEM((1, head), F32),
            pltpu.VMEM((seqs, rows, head), F32),
            pltpu.VMEM((seqs, rows, head), F32),
            pltpu.VMEM((seqs, 2, head, head), F32),
            pltpu.VMEM((seqs, 2, head, head), F32),
            pltpu.VMEM((seqs, 2, head, head), F32),
            pltpu.VMEM((seqs, head, head), F32),
            pltpu.VMEM((seqs, 8, head), F32),
            pltpu.VMEM((seqs, 8, head), F32),
            pltpu.VMEM((seqs, count, 2 * each, head), F32),
            pltpu.VMEM((seqs, 2 * each, head), F32),
            dma((8 + CHUNKS * (seqs + 4),)),
            dma((seqs, 2)),
            dma((seqs, 2)),
            dma((seqs,)),
            dma((seqs,)),
            dma,
            dma,
            dma((seqs, count)),
            dma((seqs,)),
        ],
        compiler_params=pltpu.CompilerParams(
            collective_id=0, has_side_effects=True, vmem_limit_bytes=GRANT
        ),
    )(*[x if x.shape == (1,) else pltpu.with_memory_space_constraint(x, pltpu.HBM) for x in (
        tokens,
        decoded_input,
        query_weight,
        key_weight,
        value_weight,
        gates,
        head_decay_rate,
        extra_log_decay,
        read_norm_gain.reshape(1, head),
    )]    )


def solution(mesh):
    in_specs = (
        P("grp", "sp", None),
        P("grp", None),
        P(None, "tp"),
        P(None, "tp"),
        P(None, "tp"),
        P(),
        P("tp"),
        P("grp", "tp", "sp"),
        P(),
    )
    out_specs = (P("grp", "tp", "sp", None), P("grp", "tp"))
    return jax.shard_map(
        per_device, mesh=mesh, in_specs=in_specs, out_specs=out_specs, check_vma=False
    )
```
